32 devices in a mesh: fs: 8 (over z, core), tp: 4 (over y, x).
Axes of the slice: x: 2, y: 2, z: 4, core: 2. Of those that a mesh axis runs over, the one named last changes fastest.
Arguments:
- attn_out: bfloat16 [12288, 2048], P('fs', 'tp'), may hold values from -6 to 6
- out_cot: bfloat16 [12288, 4096], P('fs', 'tp'), may hold values from -6 to 6
- latent: bfloat16 [12288, 1024], P('fs', 'tp'), may hold values from -6 to 6
- value_cot: bfloat16 [12288, 2048], P('fs', 'tp'), may hold values from -6 to 6
- out_weight: float32 [2048, 4096], P('fs', 'tp'), may hold values from -0.125 to 0.125
- value_up_matrix: float32 [1024, 2048], P('fs', 'tp'), may hold values from -0.1875 to 0.1875
- out_basis: bfloat16 [2048, 256], P('fs'), as said below
- value_basis: bfloat16 [1024, 256], P('fs'), as said below
- out_mean: float32 [256, 4096], P(None, 'tp'), may hold values from -2660.43 to 2660.43
- out_square: float32 [256, 4096], P(None, 'tp'), may hold values from 12288 to 2457600, as said below
- value_mean: float32 [256, 2048], P(None, 'tp'), may hold values from -2660.43 to 2660.43
- value_square: float32 [256, 2048], P(None, 'tp'), may hold values from 12288 to 2457600, as said below
Outputs:
- out_step: float32 [2048, 4096], P('fs', 'tp')
- out_new: float32 [2048, 4096], P('fs', 'tp')
- out_copy: bfloat16 [2048, 4096], P(None, 'tp')
- out_mean_new: float32 [256, 4096], P(None, 'tp')
- out_square_new: float32 [256, 4096], P(None, 'tp')
- value_step: float32 [1024, 2048], P('fs', 'tp')
- value_new: float32 [1024, 2048], P('fs', 'tp')
- value_copy: bfloat16 [1024, 2048], P(None, 'tp')
- value_mean_new: float32 [256, 2048], P(None, 'tp')
- value_square_new: float32 [256, 2048], P(None, 'tp')
The draws below stay inside these ranges and needn't reach their ends.
Inputs may be any that keep to these rules, and one draw needn't show every extreme that they name: `out_basis`: factors of full rank, rows of differing scales. `value_basis`: factors of full rank, rows of differing scales. `out_square`: Positive. `value_square`: Positive.
All inputs are finite; a program needn't handle non-finite values.
Results may differ from the reference program's by a relative error of at most 0.012.
Values may be sent and summed in bfloat16 or wider, within the bound.
A program may use at most 64 MiB of HBM per device.

```python
import jax
import jax.numpy as jnp
from jax import lax

D = 4096
LATENT_WIDTH = 1024
RANK = 256
VALUE_FEATURES = 2048
TOKEN_TOTAL = 12288


def draw_out_basis(key, part):
    row_slices = VALUE_FEATURES
    index = jnp.arange(row_slices, dtype=jnp.float32) / (row_slices - 1)
    base = jnp.clip(jax.random.normal(jax.random.fold_in(key, 22), (row_slices, RANK), jnp.float32), -4.0, 4.0)
    ramp = 10.0 ** index
    return (base * ramp[:, None] * row_slices ** (-0.5)).astype(jnp.bfloat16)


def draw_value_basis(key, part):
    row_slices = LATENT_WIDTH
    index = jnp.arange(row_slices, dtype=jnp.float32) / (row_slices - 1)
    base = jnp.clip(jax.random.normal(jax.random.fold_in(key, 32), (row_slices, RANK), jnp.float32), -4.0, 4.0)
    ramp = 10.0 ** index
    return (base * ramp[:, None] * row_slices ** (-0.5)).astype(jnp.bfloat16)


def draw_out_square(key, part):
    cols = D
    index = jnp.arange(cols, dtype=jnp.float32) / (cols - 1)
    base = jnp.exp(jax.random.uniform(jax.random.fold_in(key, 42), (RANK, cols), jnp.float32, -1.2, 1.09))
    ramp = 10.0 ** (index - 0.5)
    return 20.0 * TOKEN_TOTAL * base * ramp[None, :]


def draw_value_square(key, part):
    cols = VALUE_FEATURES
    index = jnp.arange(cols, dtype=jnp.float32) / (cols - 1)
    base = jnp.exp(jax.random.uniform(jax.random.fold_in(key, 52), (RANK, cols), jnp.float32, -1.2, 1.09))
    ramp = 10.0 ** (index - 0.5)
    return 20.0 * TOKEN_TOTAL * base * ramp[None, :]


def strengthened(array, own_key, source, target, parts, factor):
    def block_of(axis_at):
        return (jnp.arange(array.shape[axis_at]) // (array.shape[axis_at] // parts)).reshape((-1,) + (1,) * (array.ndim - 1 - axis_at))

    first = jax.random.permutation(own_key, parts)[block_of(target)]
    other_side = (block_of(target) + parts // 2) % parts
    return jnp.where((block_of(source) == first) | (block_of(source) == other_side), factor * array, array)


def steps_of(key, dims, shards, smallest, largest):
    loudness = 1.0
    for position, shards_of in shards:
        draws = jax.random.uniform(jax.random.fold_in(jax.random.fold_in(key, 6), position), (shards_of,), jnp.float32, smallest / len(shards), largest / len(shards))
        loudness = loudness * jnp.repeat(jnp.exp(draws), dims[position] // shards_of).reshape((-1,) + (1,) * (len(dims) - 1 - position))
    return loudness


def noise(own_key, shape, scale, most, shards=(), kind=jnp.bfloat16):
    array = scale * jax.random.normal(own_key, shape, jnp.float32)
    if shards:
        array = array * steps_of(own_key, shape, shards, -0.22, 0.18)
    return jnp.clip(array, -most, most).astype(kind)


def noise_with(rng, extent, scale, bound, split, heavy, kind=jnp.bfloat16):
    values = scale * jax.random.normal(rng, extent, jnp.float32)
    if split:
        values = values * steps_of(rng, extent, split, -0.22, 0.18)
    return jnp.clip(strengthened(values, jax.random.fold_in(rng, 3), *heavy), -bound, bound).astype(kind)


def setup_inputs(seed: int = 0) -> dict:
    seeds = jax.random.split(jax.random.key(seed), 13)
    attn_out = noise_with(seeds[0], (TOKEN_TOTAL, VALUE_FEATURES), 1.0, 6.0, ((0, 8), (1, 4)), (0, 1, 8, 2.0))
    out_cot = noise(seeds[1], (TOKEN_TOTAL, D), 1.0, 6.0, ((0, 8), (1, 4)))
    latent = noise_with(seeds[2], (TOKEN_TOTAL, LATENT_WIDTH), 1.0, 6.0, ((0, 8), (1, 4)), (0, 1, 8, 2.0))
    value_cot = noise(seeds[3], (TOKEN_TOTAL, VALUE_FEATURES), 1.0, 6.0, ((0, 8), (1, 4)))
    out_weight = noise(seeds[4], (VALUE_FEATURES, D), VALUE_FEATURES ** -0.5, 0.125, ((0, 8), (1, 4)), jnp.float32)
    value_up_matrix = noise(seeds[5], (LATENT_WIDTH, VALUE_FEATURES), LATENT_WIDTH ** -0.5, 0.1875, ((0, 8), (1, 4)), jnp.float32)
    out_basis = draw_out_basis(jax.random.fold_in(seeds[12], 71), 0)
    value_basis = draw_value_basis(jax.random.fold_in(seeds[12], 71), 0)
    out_mean = noise(seeds[8], (RANK, D), (4 * TOKEN_TOTAL ** 0.5), 2660.43, ((1, 4),), jnp.float32)
    out_square = draw_out_square(jax.random.fold_in(seeds[12], 71), 0)
    value_mean = noise(seeds[10], (RANK, VALUE_FEATURES), (4 * TOKEN_TOTAL ** 0.5), 2660.43, ((1, 4),), jnp.float32)
    value_square = draw_value_square(jax.random.fold_in(seeds[12], 71), 0)
    return {"attn_out": attn_out, "out_cot": out_cot, "latent": latent, "value_cot": value_cot, "out_weight": out_weight, "value_up_matrix": value_up_matrix, "out_basis": out_basis, "value_basis": value_basis, "out_mean": out_mean, "out_square": out_square, "value_mean": value_mean, "value_square": value_square}


LEARN_RATE = 0.01
MEAN_DECAY = 0.8
BETA_SQUARE = 0.9
EPS_RMS = 1e-06

def adapt(grad, basis, mean_in, square_in, weight_in):
    basis_f = basis.astype(jnp.float32)
    proj = jnp.dot(basis_f.T, grad, precision=lax.Precision.HIGHEST)
    mean_new = MEAN_DECAY * mean_in + (1.0 - MEAN_DECAY) * proj
    square_new = BETA_SQUARE * square_in + (1.0 - BETA_SQUARE) * proj * proj
    direction = mean_new / jnp.sqrt(square_new)
    update_delta = jnp.dot(basis_f, direction, precision=lax.Precision.HIGHEST)
    total = jnp.sum(update_delta * update_delta)
    count = update_delta.shape[0] * update_delta.shape[1]
    step = LEARN_RATE * update_delta * lax.rsqrt(total / count + EPS_RMS)
    weight_new = weight_in - step
    return (step, weight_new, weight_new.astype(jnp.bfloat16), mean_new, square_new)

def reference(attn_out, out_cot, latent, value_cot, out_weight, value_up_matrix, out_basis, value_basis, out_mean, out_square, value_mean, value_square):
    grad_out = jnp.dot(attn_out.T, out_cot, preferred_element_type=jnp.float32)
    grad_value = jnp.dot(latent.T, value_cot, preferred_element_type=jnp.float32)
    first = adapt(grad_out, out_basis, out_mean, out_square, out_weight)
    second = adapt(grad_value, value_basis, value_mean, value_square, value_up_matrix)
    return (first[0], first[1], first[2], first[3], first[4], second[0], second[1], second[2], second[3], second[4])
```

```python
import functools

import jax
import jax.numpy as jnp
from jax import lax
from jax.experimental import pallas as pl
from jax.experimental.pallas import tpu as pltpu
from jax.sharding import PartitionSpec as P

LEARN_RATE = 0.01
MEAN_DECAY = 0.8
BETA_SQUARE = 0.9
EPS_RMS = 1e-06
MESH = pl.DeviceIdType.MESH
F32, BF16 = jnp.float32, jnp.bfloat16
PAIR = (0, 1)
CORES = 2
NEAR = (((1, 0),), ((1, 1), (1, 2)), ((2, 0),), ((2, 1),), ((2, 2),))


def rcopy(src, dst, send, recv, fs, tp):
    return pltpu.make_async_remote_copy(
        src_ref=src, dst_ref=dst, send_sem=send, recv_sem=recv,
        device_id=(fs, tp), device_id_type=MESH,
    )


def over_rows(left, right):
    return lax.dot_general(left, right, (((0,), (0,)), ((), ())), preferred_element_type=F32)


def exchange(nf, nt, *refs):
    hbm, rest = refs[:12], refs[12:]
    wg, bg, dirs, mean_new, square_new, w32 = (rest[2 * k:2 * k + 2] for k in range(6))
    totals, rest = rest[12], rest[13:]
    left, right, mean, square, sbuf, rbuf, kept, lifted, part, psend, pbuf, zsend, zbuf, tot, gram = (
        rest[2 * k:2 * k + 2] for k in range(15))
    (tsend, tbuf, isem, b_s, b_r, bd_s, bd_r, c_s, c_r, w_u, w_d, w_r, wd_s, wd_r,
     rs_s, rs_r, ag_s, ag_r, p_s, p_r, z_s, z_r, g_s, g_r, gd_s, gd_r, t_s, t_r) = rest[30:]

    nz = nf // CORES
    f, t = lax.axis_index("fs"), lax.axis_index("tp")
    z, c = lax.div(f, CORES), lax.rem(f, CORES)
    partner = f + 1 - 2 * c
    rank = bg[0].shape[2]
    tokens, seg = left[0].shape[0], rank // nf
    peers_t = [lax.rem(t + s, nt) for s in range(1, nt)]
    peers_z = [lax.rem(z + s, nz) for s in range(1, nz)]
    own_column = z == t

    held = (*left, *right, *w32, *[b.at[f] for b in bg], *mean, *square)
    order = (6, 7, 4, 5, 0, 1, 2, 3, 8, 9, 10, 11)
    fetch = [pltpu.make_async_copy(hbm[k], held[k], isem.at[k]) for k in range(12)]
    for k in order:
        fetch[k].start()

    barrier = pltpu.get_barrier_semaphore()
    pl.semaphore_signal(barrier, inc=1, device_id=(partner, t), device_id_type=MESH)
    for pz in peers_z:
        pl.semaphore_signal(barrier, inc=1, device_id=(pz * CORES + c, t), device_id_type=MESH)
    for pt in peers_t:
        pl.semaphore_signal(barrier, inc=1, device_id=(f, pt), device_id_type=MESH)
    pl.semaphore_wait(barrier, 1 + len(peers_z) + len(peers_t))

    lane = t * CORES + c
    other = t * CORES + 1 - c

    def basis_line(i, zz):
        block = bg[i].at[lane]
        return rcopy(block, block, b_s.at[i, zz], b_r.at[i], zz * CORES + c, t)

    def basis_core(i, block):
        ref = bg[i].at[block]
        return rcopy(ref, ref, bd_s.at[i, block], bd_r.at[i, block], partner, t)

    def basis_plane(i, pt, block):
        ref = bg[i].at[block]
        return rcopy(ref, ref, c_s.at[i, pt], c_r.at[i, lax.div(block, CORES)], f, pt)

    for i in PAIR:
        fetch[6 + i].wait()

        @pl.when(own_column)
        def _():
            for dist in range(nz - 1, 0, -1):
                for zz, there in ((z + dist, z + dist < nz), (z - dist, z - dist >= 0)):
                    @pl.when(there)
                    def _():
                        basis_line(i, zz).start()
        basis_core(i, f).start()
    for i in PAIR:
        fetch[4 + i].wait()
        wg[i][f] = w32[i][...].astype(BF16)

    heights = [w.shape[1] for w in wg]
    tall = min(heights)
    units = [(i, r) for i in PAIR for r in range(0, heights[i], tall)]

    def unit(u, zb, core):
        i, r = units[u]
        return wg[i].at[zb * CORES + core, pl.ds(r, tall)]

    def w_up(u, zb):
        ref = unit(u, zb, c)
        return rcopy(ref, ref, w_u.at[u, zb], w_r.at[u, zb], f + CORES, t)

    def w_dn(u, zb):
        ref = unit(u, zb, c)
        return rcopy(ref, ref, w_d.at[u, zb], w_r.at[u, zb], f - CORES, t)

    def w_core(u, zb, core):
        ref = unit(u, zb, core)
        return rcopy(ref, ref, wd_s.at[u, zb], wd_r.at[u, zb], partner, t)

    def pass_on(u, zb, up, down):
        if up:
            @pl.when(z < nz - 1)
            def _():
                w_up(u, zb).start()
        if down:
            @pl.when(z > 0)
            def _():
                w_dn(u, zb).start()

    def weights_on(events):
        for s, u in events:
            if s > nz - 1:
                continue

            @pl.when(z >= s)
            def _():
                w_up(u, z - s).wait_recv()
                pass_on(u, z - s, True, False)
                w_core(u, z - s, c).start()

            @pl.when(z + s <= nz - 1)
            def _():
                w_dn(u, z + s).wait_recv()
                pass_on(u, z + s, False, True)
                w_core(u, z + s, c).start()

    for i in PAIR:
        @pl.when(jnp.logical_not(own_column))
        def _():
            basis_line(i, z).wait_recv()
            basis_core(i, lane).start()
        if i == 0:
            for u in range(len(units)):
                pass_on(u, z, True, True)

    levels = nt.bit_length() - 1
    sizes = [tokens // 2 >> k for k in range(levels + 1)]
    offs = [sizes[0] - s for s in sizes]
    masks = [[1 << k for k in range(levels)], [1 << k for k in reversed(range(levels))]]
    bits = [[lax.rem(lax.div(t, m), 2) for m in masks[h]] for h in PAIR]
    mates = [[t + m * (1 - 2 * b) for m, b in zip(masks[h], bits[h])] for h in PAIR]
    bases = []
    for h in PAIR:
        at = [h * sizes[0]]
        for k in range(levels):
            at.append(at[-1] + bits[h][k] * sizes[k + 1])
        bases.append(at)

    def rows(start, size):
        return pl.ds(pl.multiple_of(start, 16), size)

    def away(h, k):
        return rows(bases[h][k] + (1 - bits[h][k]) * sizes[k + 1], sizes[k + 1])

    def rs(i, h, k):
        at = pl.ds(offs[k], sizes[k + 1])
        return rcopy(sbuf[i].at[h, at], rbuf[i].at[h, at], rs_s.at[i, h, k], rs_r.at[i, h, k], f, mates[h][k])

    def ag(i, h, k, received=False):
        ref = lifted[i].at[away(h, k) if received else rows(bases[h][k + 1], sizes[k + 1])]
        return rcopy(ref, ref, ag_s.at[i, h, k], ag_r.at[i, h, k], f, mates[h][k])

    def lift_tokens(i):
        two = bg[i][pl.ds(t * CORES, CORES)]
        factor = two.reshape(two.shape[0] * two.shape[1], rank)
        for h in PAIR:
            sbuf[i][h, pl.ds(0, sizes[1])] = jnp.dot(
                left[i][away(h, 0), :], factor, preferred_element_type=F32).astype(BF16)
            rs(i, h, 0).start()
        for h in PAIR:
            kept[i][h, pl.ds(0, sizes[1])] = jnp.dot(
                left[i][rows(bases[h][1], sizes[1]), :], factor, preferred_element_type=F32)

    def contract(i, at, first=False):
        got = over_rows(lifted[i][at, :], right[i][at, :])
        if first:
            part[i][...] = got
        else:
            part[i][...] += got

    def halve(i, k):
        for h in PAIR:
            rs(i, h, k).wait_recv()
            if k + 1 < levels:
                small = sizes[k + 2]
                for b, mine in ((1 - bits[h][k + 1], False), (bits[h][k + 1], True)):
                    at = rows(offs[k] + b * small, small)
                    both = kept[i][h, at] + rbuf[i][h, at].astype(F32)
                    to = pl.ds(offs[k + 1], small)
                    if mine:
                        kept[i][h, to] = both
                    else:
                        sbuf[i][h, to] = both.astype(BF16)
                        rs(i, h, k + 1).start()
            else:
                at = pl.ds(offs[k], sizes[k + 1])
                lifted[i][rows(bases[h][k + 1], sizes[k + 1]), :] = (
                    kept[i][h, at] + rbuf[i][h, at].astype(F32)).astype(BF16)
                ag(i, h, k).start()
        if k + 1 == levels:
            fetch[2 + i].wait()
            for h in PAIR:
                contract(i, rows(bases[h][levels], sizes[levels]), h == 0)

    def double(i, k):
        for h in PAIR:
            ag(i, h, k, True).wait_recv()
            if k > 0:
                ag(i, h, k - 1).start()
        for h in PAIR:
            contract(i, away(h, k))

    def piece(i, core, zz):
        return part[i][pl.ds(pl.multiple_of((core * nz + zz) * seg, seg), seg), :]

    pairs = [rcopy(psend[i], pbuf[i], p_s.at[i], p_r.at[i], partner, t) for i in PAIR]
    me = c * nz + z

    def pair_send(i):
        for zz in range(nz):
            psend[i][zz] = piece(i, 1 - c, zz).astype(BF16)
        pairs[i].start()

    def line(i, pz):
        return rcopy(zsend[i].at[pz], zbuf[i].at[z], z_s.at[i, pz], z_r.at[i, z], pz * CORES + c, t)

    def line_got(i, pz):
        return rcopy(zsend[i].at[pz], zbuf[i].at[pz], z_s.at[i, pz], z_r.at[i, pz], pz * CORES + c, t)

    def share(i, pz, at):
        ref = tot[i].at[at]
        return rcopy(ref, ref, g_s.at[i, pz], g_r.at[i, at - c * nz], pz * CORES + c, t)

    def share_core(i, core, zz):
        ref = tot[i].at[core * nz + zz]
        return rcopy(ref, ref, gd_s.at[i, zz], gd_r.at[i, zz], partner, t)

    def line_send(i):
        pairs[i].wait_recv()
        for pz in peers_z:
            zsend[i][pz] = (piece(i, c, pz) + pbuf[i][pz].astype(F32)).astype(BF16)
            line(i, pz).start()

    def line_sum(i):
        acc = piece(i, c, z) + pbuf[i][z].astype(F32)
        for pz in peers_z:
            line_got(i, pz).wait_recv()
            acc = acc + zbuf[i][pz].astype(F32)
        tot[i][me] = acc.astype(BF16)
        for pz in peers_z:
            share(i, pz, me).start()
        share_core(i, c, z).start()

    def line_take(i):
        for pz in peers_z:
            share(i, pz, c * nz + pz).wait_recv()
            share_core(i, c, pz).start()

    def squared(i):
        flat = bg[i][...].reshape(nf * bg[i].shape[1], rank)
        full = over_rows(flat, flat)
        high = full.astype(BF16)
        gram[i][0] = high
        gram[i][1] = (full - high.astype(F32)).astype(BF16)

    def direct(i):
        for zz in range(nz):
            share_core(i, 1 - c, zz).wait_recv()
        proj = tot[i][...].astype(F32).reshape(part[i].shape)
        mean_out = MEAN_DECAY * mean[i][...] + (1.0 - MEAN_DECAY) * proj
        square_out = BETA_SQUARE * square[i][...] + (1.0 - BETA_SQUARE) * proj * proj
        mean_new[i][...] = mean_out
        square_new[i][...] = square_out
        d = (mean_out / jnp.sqrt(square_out)).astype(BF16)
        dirs[i][...] = d
        turned = (jnp.dot(gram[i][0], d, preferred_element_type=F32)
                  + jnp.dot(gram[i][1], d, preferred_element_type=F32))
        sums = jnp.sum(d.astype(F32) * turned, axis=0, keepdims=True)
        tile = jnp.zeros((8, 128), F32) + jnp.sum(sums, axis=1, keepdims=True)
        tsend[i] = tile
        tbuf[t, i] = tile

    def plane_send(i):
        @pl.when(jnp.logical_not(own_column))
        def _():
            for pt in peers_t:
                basis_plane(i, pt, lane).start()

    def plane_take(i):
        for pt in peers_t:
            @pl.when(pt != z)
            def _():
                basis_plane(i, pt, pt * CORES + c).wait_recv()
                basis_core(i, pt * CORES + c).start()
        for pt in peers_t:
            basis_core(i, pt * CORES + 1 - c).wait_recv()

    for i in PAIR:
        fetch[i].wait()
        basis_core(i, other).wait_recv()
        lift_tokens(i)
    for u in range(len(units)):
        w_core(u, z, c).start()

    points = list(NEAR)
    for k in range(levels):
        for i in PAIR:
            halve(i, k)
            if k < 1:
                weights_on(points.pop(0))
    weights_on(points.pop(0))
    for k in range(levels - 1, 0, -1):
        for i in PAIR:
            double(i, k)
    double(0, 0)
    pair_send(0)
    line_send(0)
    weights_on(points.pop(0))
    double(1, 0)
    pair_send(1)
    line_send(1)
    for i in PAIR:
        plane_send(i)
    line_sum(0)
    line_sum(1)
    weights_on(points.pop(0))
    for i in PAIR:
        plane_take(i)
        squared(i)
    for i in PAIR:
        fetch[8 + i].wait()
        fetch[10 + i].wait()
    for i in PAIR:
        line_take(i)
    for i in PAIR:
        direct(i)
    for pt in peers_t:
        rcopy(tsend, tbuf.at[t], t_s.at[pt], t_r.at[t], f, pt).start()
    weights_on([(s, u) for s in range(3, nz) for u in range(len(units))])

    for pt in peers_t:
        rcopy(tsend, tbuf.at[pt], t_s.at[pt], t_r.at[pt], f, pt).wait_recv()
    summed = tbuf[0]
    for k in range(1, nt):
        summed = summed + tbuf[k]
    totals[...] = summed

    for u in range(len(units)):
        for zb in range(nz):
            w_core(u, zb, 1 - c).wait_recv()
    for i in PAIR:
        @pl.when(own_column)
        def _():
            for pz in peers_z:
                basis_line(i, pz).wait_send()

        @pl.when(jnp.logical_not(own_column))
        def _():
            basis_core(i, lane).wait_send()
            for pt in peers_t:
                basis_plane(i, pt, lane).wait_send()
        basis_core(i, f).wait_send()
        for pt in peers_t:
            @pl.when(pt != z)
            def _():
                basis_core(i, pt * CORES + c).wait_send()
        for h in PAIR:
            for k in range(levels):
                rs(i, h, k).wait_send()
                ag(i, h, k).wait_send()
        pairs[i].wait_send()
        for pz in peers_z:
            line(i, pz).wait_send()
            share(i, pz, me).wait_send()
        for zz in range(nz):
            share_core(i, c, zz).wait_send()
    for u in range(len(units)):
        for zb in range(nz):
            w_core(u, zb, c).wait_send()

            @pl.when((z >= zb) & (z < nz - 1))
            def _():
                w_up(u, zb).wait_send()

            @pl.when((z <= zb) & (z > 0))
            def _():
                w_dn(u, zb).wait_send()
    for pt in peers_t:
        rcopy(tsend, tbuf.at[t], t_s.at[pt], t_r.at[t], f, pt).wait_send()


def gather_and_reduce(nf, nt, lefts, rights, weights, bases, means, squares):
    rank, nz, tokens = bases[0].shape[1], nf // CORES, rights[0].shape[0]
    seg, levels = rank // nf, nt.bit_length() - 1
    heights, widths = [b.shape[0] for b in bases], [r.shape[1] for r in rights]
    units = sum(heights) // min(heights)
    vmem, dma = pl.BlockSpec(memory_space=pltpu.VMEM), pltpu.SemaphoreType.DMA
    hbm = pl.BlockSpec(memory_space=pltpu.HBM)

    def two(shape_of, kind=BF16, make=pltpu.VMEM):
        return [make(shape_of(h, w), kind) for h, w in zip(heights, widths)]

    def outs(shape_of, kind=BF16):
        return two(shape_of, kind, jax.ShapeDtypeStruct)

    halves = lambda h, w: (2, tokens // 2, rank)
    line_pieces = lambda h, w: (nz, seg, w)
    ranked = lambda h, w: (rank, w)
    fetched = (*lefts, *rights, *means, *squares)
    return pl.pallas_call(
        functools.partial(exchange, nf, nt),
        out_shape=(
            *outs(lambda h, w: (nf, h, w)), *outs(lambda h, w: (nf, h, rank)), *outs(ranked),
            *outs(ranked, F32), *outs(ranked, F32), *outs(lambda h, w: (h, w), F32),
            jax.ShapeDtypeStruct((2, 8, 128), F32),
        ),
        in_specs=[hbm] * 12,
        out_specs=(vmem,) * 13,
        scratch_shapes=[
            *[pltpu.VMEM(x.shape, x.dtype) for x in fetched],
            *two(halves), *two(halves), *two(halves, F32), *two(lambda h, w: (tokens, rank)), *two(ranked, F32),
            *two(line_pieces), *two(line_pieces), *two(line_pieces), *two(line_pieces),
            *two(lambda h, w: (nf, seg, w)), *two(lambda h, w: (2, rank, rank)),
            pltpu.VMEM((2, 8, 128), F32),
            pltpu.VMEM((nt, 2, 8, 128), F32),
            dma((12,)), dma((2, nz)), dma((2,)), dma((2, nf)), dma((2, nf)), dma((2, nt)), dma((2, nt)),
            *[dma((units, nz))] * 5,
            *[dma((2, 2, levels))] * 4,
            dma((2,)), dma((2,)), *[dma((2, nz))] * 6, dma((nt,)), dma((nt,)),
        ],
        compiler_params=pltpu.CompilerParams(
            collective_id=0, has_side_effects=True, vmem_limit_bytes=40 * 1024 * 1024
        ),
        name="exchange",
    )(*[pltpu.with_memory_space_constraint(x, pltpu.HBM)
        for x in (*lefts, *rights, *weights, *bases, *means, *squares)])


def apply(nf, nt, *refs):
    wg, bg, dirs, mean_new, square_new, w32 = (refs[2 * k:2 * k + 2] for k in range(6))
    totals = refs[12]
    outs = [refs[13 + 5 * i:18 + 5 * i] for i in PAIR]
    step, new, copy = (refs[23 + 2 * k:25 + 2 * k] for k in range(3))
    sem, csem = refs[29:]
    f = lax.axis_index("fs")

    def to(k, i):
        src = (step, new, None, mean_new, square_new)[k]
        return pltpu.make_async_copy(src[i], outs[i][k], sem.at[i, k])

    def block(i, g):
        height = w32[i].shape[0]
        return pltpu.make_async_copy(copy[i].at[pl.ds(g * height, height)],
                                     outs[i][2].at[pl.ds(g * height, height)], csem.at[i, g])

    for i in PAIR:
        to(3, i).start()
        to(4, i).start()
    scales = []
    for i in PAIR:
        count = w32[i].shape[0] * nf * w32[i].shape[1] * nt
        scale = LEARN_RATE * lax.rsqrt(totals[i, 0:1, 0:1] / lax.convert_element_type(count, F32) + EPS_RMS)
        scales.append(scale)
        own = scale * jnp.dot(bg[i][f], dirs[i][...], preferred_element_type=F32)
        step[i][...] = own
        new[i][...] = w32[i][...] - own
        to(0, i).start()
        to(1, i).start()
    for i in PAIR:
        height = w32[i].shape[0]
        for g in range(nf):
            update = jnp.dot(bg[i][g], dirs[i][...], preferred_element_type=F32)
            copy[i][pl.ds(g * height, height), :] = (wg[i][g].astype(F32) - scales[i] * update).astype(BF16)
            block(i, g).start()
    for i in PAIR:
        for k in (0, 1, 3, 4):
            to(k, i).wait()
        for g in range(nf):
            block(i, g).wait()


def finish(nf, nt, gathered):
    w32 = gathered[10:12]
    vmem, hbm = pl.BlockSpec(memory_space=pltpu.VMEM), pl.BlockSpec(memory_space=pltpu.HBM)
    out_shape = []
    for i in PAIR:
        copy = jax.ShapeDtypeStruct((nf * w32[i].shape[0], w32[i].shape[1]), BF16)
        like = lambda x: jax.ShapeDtypeStruct(x.shape, F32)
        out_shape += [like(w32[i]), like(w32[i]), copy, like(gathered[6 + i]), like(gathered[8 + i])]
    return pl.pallas_call(
        functools.partial(apply, nf, nt),
        in_specs=[vmem] * 13,
        out_specs=[hbm] * 10,
        out_shape=out_shape,
        scratch_shapes=[
            *[pltpu.VMEM(w.shape, F32) for w in w32], *[pltpu.VMEM(w.shape, F32) for w in w32],
            *[pltpu.VMEM(out_shape[2 + 5 * i].shape, BF16) for i in PAIR],
            pltpu.SemaphoreType.DMA((2, 5)), pltpu.SemaphoreType.DMA((2, nf)),
        ],
        compiler_params=pltpu.CompilerParams(vmem_limit_bytes=12 * 1024 * 1024),
        name="apply",
    )(*gathered)


def per_device(nf, nt, attn_out, out_cot, latent, value_cot, out_weight, value_up_matrix,
               out_basis, value_basis, out_mean, out_square, value_mean, value_square):
    gathered = gather_and_reduce(
        nf, nt, (attn_out, latent), (out_cot, value_cot), (out_weight, value_up_matrix),
        (out_basis, value_basis), (out_mean, value_mean), (out_square, value_square))
    return tuple(finish(nf, nt, gathered))


def solution(mesh):
    both, rows, cols = P("fs", "tp"), P("fs", None), P(None, "tp")
    return jax.shard_map(
        functools.partial(per_device, mesh.shape["fs"], mesh.shape["tp"]),
        mesh=mesh,
        in_specs=(both,) * 6 + (rows,) * 2 + (cols,) * 4,
        out_specs=(both, both, cols, cols, cols) * 2,
        check_vma=False,
    )
```

```python
import functools

import jax
import jax.numpy as jnp
from jax import lax
from jax.experimental import pallas as pl
from jax.experimental.pallas import tpu as pltpu
from jax.sharding import PartitionSpec as P

LEARN_RATE = 0.01
MEAN_DECAY = 0.8
BETA_SQUARE = 0.9
EPS_RMS = 1e-06
MESH = pl.DeviceIdType.MESH
F32, BF16 = jnp.float32, jnp.bfloat16
PAIR = (0, 1)
CORES = 2
NEAR = (((1, 0), (1, 1)), ((1, 2),), ((1, 3), (1, 4)), ((2, 0),), ((2, 1),), ((2, 2),), ((2, 3),), ((2, 4),))


def rcopy(src, dst, send, recv, fs, tp):
    return pltpu.make_async_remote_copy(
        src_ref=src, dst_ref=dst, send_sem=send, recv_sem=recv,
        device_id=(fs, tp), device_id_type=MESH,
    )


def over_rows(left, right):
    return lax.dot_general(left, right, (((0,), (0,)), ((), ())), preferred_element_type=F32)


def unit_heights(heights, widths):
    least = min(h * w for h, w in zip(heights, widths))
    return [least // w for w in widths]


def parts_of(height, nt):
    return min(nt, height // 16)


def exchange(nf, nt, *refs):
    hbm, rest = refs[:12], refs[12:]
    wg, bg, dirs, mean_new, square_new, w32 = (rest[2 * k:2 * k + 2] for k in range(6))
    totals, rest = rest[12], rest[13:]
    left, right, mean, square = (rest[2 * k:2 * k + 2] for k in range(4))
    sbuf, rbuf, kept, lifted, part, psend, pbuf, zsend, zbuf, tot = (rest[8 + 4 * k:12 + 4 * k] for k in range(10))
    (tsend, tbuf, isem, b_s, b_r, bd_s, bd_r, c_s, c_r, e_s, e_r, cd_s, cd_r, w_u, w_d, w_r, wd_s, wd_r,
     rs_s, rs_r, ag_s, ag_r, p_s, p_r, z_s, z_r, g_s, g_r, gd_s, gd_r, t_s, t_r) = rest[48:]

    nz = nf // CORES
    f, t = lax.axis_index("fs"), lax.axis_index("tp")
    z, c = lax.div(f, CORES), lax.rem(f, CORES)
    partner = f + 1 - 2 * c
    rank = bg[0].shape[2]
    half = rank // 2
    tokens = left[0].shape[0]
    peers_t = [lax.rem(t + s, nt) for s in range(1, nt)]
    peers_z = [lax.rem(z + s, nz) for s in range(1, nz)]
    own_column = z == t
    elsewhere = jnp.logical_not(own_column)

    held = (*left, *right, *w32, *[b.at[f] for b in bg], *mean, *square)
    order = (6, 7, 4, 5, 0, 1, 2, 3, 8, 9, 10, 11)
    fetch = [pltpu.make_async_copy(hbm[k], held[k], isem.at[k]) for k in range(12)]
    for k in order:
        fetch[k].start()

    barrier = pltpu.get_barrier_semaphore()
    pl.semaphore_signal(barrier, inc=1, device_id=(partner, t), device_id_type=MESH)
    for pz in peers_z:
        pl.semaphore_signal(barrier, inc=1, device_id=(pz * CORES + c, t), device_id_type=MESH)
    for pt in peers_t:
        pl.semaphore_signal(barrier, inc=1, device_id=(f, pt), device_id_type=MESH)
    pl.semaphore_wait(barrier, 1 + len(peers_z) + len(peers_t))

    lane = t * CORES + c
    other = t * CORES + 1 - c
    chunks = ((0, 0, half), (0, half, half), (1, 0, rank))

    def slab(i, block, column, first=0, size=rank):
        tall = bg[i].shape[1] // parts_of(bg[i].shape[1], nt)
        return bg[i].at[block, pl.ds(pl.multiple_of(column * tall, tall), tall), pl.ds(first, size)]

    def when_part(i, column, then):
        parts = parts_of(bg[i].shape[1], nt)
        if parts == nt:
            then()
        else:
            pl.when(column < parts)(then)

    def basis_line(k, pz, block):
        i, first, size = chunks[k]
        ref = slab(i, block, t, first, size)
        return rcopy(ref, ref, b_s.at[k, pz], b_r.at[k, lax.div(block, CORES)], pz * CORES + c, t)

    def basis_plane(k, b, column):
        i, first, size = chunks[k]
        ref = slab(i, b * CORES + c, column, first, size)
        return rcopy(ref, ref, c_s.at[k, b], c_r.at[k, column], f, b)

    def basis_core(k, block):
        i, first, size = chunks[k]
        ref = bg[i].at[block, :, pl.ds(first, size)]
        return rcopy(ref, ref, bd_s.at[k], bd_r.at[k], partner, t)

    def rest_plane(i, b, column, pt):
        ref = slab(i, b * CORES + c, column)
        return rcopy(ref, ref, e_s.at[i, b, pt], e_r.at[i, b, column], f, pt)

    def rest_core(i, block):
        ref = bg[i].at[block]
        return rcopy(ref, ref, cd_s.at[i, block], cd_r.at[i, block], partner, t)

    heights = [w.shape[1] for w in wg]
    tall = unit_heights(heights, [w.shape[2] for w in wg])
    units = [(i, r) for i in PAIR for r in range(0, heights[i], tall[i])]

    def unit(u, zb, core):
        i, r = units[u]
        return wg[i].at[zb * CORES + core, pl.ds(r, tall[i])]

    def w_up(u, zb):
        ref = unit(u, zb, c)
        return rcopy(ref, ref, w_u.at[u, zb], w_r.at[u, zb], f + CORES, t)

    def w_dn(u, zb):
        ref = unit(u, zb, c)
        return rcopy(ref, ref, w_d.at[u, zb], w_r.at[u, zb], f - CORES, t)

    def w_core(u, zb, core):
        ref = unit(u, zb, core)
        return rcopy(ref, ref, wd_s.at[u, zb], wd_r.at[u, zb], partner, t)

    def weights_on(events):
        for s, u in events:
            if s > nz - 1:
                continue

            @pl.when(z >= s)
            def _():
                w_up(u, z - s).wait_recv()

                @pl.when(z < nz - 1)
                def _():
                    w_up(u, z - s).start()
                w_core(u, z - s, c).start()

            @pl.when(z + s <= nz - 1)
            def _():
                w_dn(u, z + s).wait_recv()

                @pl.when(z > 0)
                def _():
                    w_dn(u, z + s).start()
                w_core(u, z + s, c).start()

    fetch[6].wait()
    fetch[7].wait()
    for k in range(len(chunks)):
        def to_line(k=k):
            for pz in [lax.rem(z + s, nz) for s in range(nz // 2, nz)] + [lax.rem(z + s, nz) for s in range(1, nz // 2)]:
                basis_line(k, pz, f).start()
        when_part(chunks[k][0], t, to_line)

    @pl.when(own_column)
    def _():
        for k in range(len(chunks)):
            basis_core(k, lane).start()
    for i in PAIR:
        fetch[4 + i].wait()
        wg[i][f] = w32[i][...].astype(BF16)
    for u in range(len(units)):
        @pl.when(z < nz - 1)
        def _():
            w_up(u, z).start()

        @pl.when(z > 0)
        def _():
            w_dn(u, z).start()

    levels = nt.bit_length() - 1
    sizes = [tokens // 2 >> k for k in range(levels + 1)]
    offs = [sizes[0] - s for s in sizes]
    masks = [[1 << k for k in range(levels)], [1 << k for k in reversed(range(levels))]]
    bits = [[lax.rem(lax.div(t, m), 2) for m in masks[h]] for h in PAIR]
    mates = [[t + m * (1 - 2 * b) for m, b in zip(masks[h], bits[h])] for h in PAIR]
    bases = []
    for h in PAIR:
        at = [h * sizes[0]]
        for k in range(levels):
            at.append(at[-1] + bits[h][k] * sizes[k + 1])
        bases.append(at)
    streams = tuple((i, r) for i in PAIR for r in PAIR)

    def rows(start, size):
        return pl.ds(pl.multiple_of(start, 16), size)

    def away(h, k):
        return rows(bases[h][k] + (1 - bits[h][k]) * sizes[k + 1], sizes[k + 1])

    def rs(q, h, k):
        at = pl.ds(offs[k], sizes[k + 1])
        return rcopy(sbuf[q].at[h, at], rbuf[q].at[h, at], rs_s.at[q, h, k], rs_r.at[q, h, k], f, mates[h][k])

    def ag(q, h, k, received=False):
        ref = lifted[q].at[away(h, k) if received else rows(bases[h][k + 1], sizes[k + 1])]
        return rcopy(ref, ref, ag_s.at[q, h, k], ag_r.at[q, h, k], f, mates[h][k])

    def basis_in(k):
        def from_line():
            for b in peers_z:
                basis_line(k, b, b * CORES + c).wait_recv()

                @pl.when(b != t)
                def _():
                    basis_plane(k, b, t).start()

        when_part(chunks[k][0], t, from_line)

    def basis_joined(k):
        @pl.when(elsewhere)
        def _():
            for pt in peers_t:
                when_part(chunks[k][0], pt, lambda: basis_plane(k, t, pt).wait_recv())
            basis_core(k, lane).start()

    def lift(q):
        i, r = streams[q]
        two = bg[i][pl.ds(t * CORES, CORES), :, r * half:(r + 1) * half]
        factor = two.reshape(two.shape[0] * two.shape[1], half)
        for h in PAIR:
            sbuf[q][h, pl.ds(0, sizes[1])] = jnp.dot(
                left[i][away(h, 0), :], factor, preferred_element_type=F32).astype(BF16)
            rs(q, h, 0).start()
        for h in PAIR:
            kept[q][h, pl.ds(0, sizes[1])] = jnp.dot(
                left[i][rows(bases[h][1], sizes[1]), :], factor, preferred_element_type=F32)

    def contract(q, at, first=False):
        i = streams[q][0]
        got = over_rows(lifted[q][at, :], right[i][at, :]).reshape(part[q].shape)
        if first:
            part[q][...] = got
        else:
            part[q][...] += got

    def halve(q, k):
        for h in PAIR:
            rs(q, h, k).wait_recv()
            if k + 1 < levels:
                small = sizes[k + 2]
                for b, mine in ((1 - bits[h][k + 1], False), (bits[h][k + 1], True)):
                    at = rows(offs[k] + b * small, small)
                    both = kept[q][h, at] + rbuf[q][h, at].astype(F32)
                    to = pl.ds(offs[k + 1], small)
                    if mine:
                        kept[q][h, to] = both
                    else:
                        sbuf[q][h, to] = both.astype(BF16)
                        rs(q, h, k + 1).start()
            else:
                at = pl.ds(offs[k], sizes[k + 1])
                lifted[q][rows(bases[h][k + 1], sizes[k + 1]), :] = (
                    kept[q][h, at] + rbuf[q][h, at].astype(F32)).astype(BF16)
                ag(q, h, k).start()
        if k + 1 == levels:
            i, r = streams[q]
            if r == 0:
                fetch[2 + i].wait()
            for h in PAIR:
                contract(q, rows(bases[h][levels], sizes[levels]), h == 0)

    def double(q, k):
        for h in PAIR:
            ag(q, h, k, True).wait_recv()
            if k > 0:
                ag(q, h, k - 1).start()
        for h in PAIR:
            contract(q, away(h, k))

    pairs = [rcopy(psend[q], pbuf[q], p_s.at[q], p_r.at[q], partner, t) for q in range(4)]
    me = c * nz + z

    def line(q, pz):
        return rcopy(zsend[q].at[pz], zbuf[q].at[z], z_s.at[q, pz], z_r.at[q, z], pz * CORES + c, t)

    def line_got(q, pz):
        return rcopy(zsend[q].at[pz], zbuf[q].at[pz], z_s.at[q, pz], z_r.at[q, pz], pz * CORES + c, t)

    def share(q, pz, at):
        ref = tot[q].at[at]
        return rcopy(ref, ref, g_s.at[q, pz], g_r.at[q, at - c * nz], pz * CORES + c, t)

    def share_core(q, core, zz):
        ref = tot[q].at[core * nz + zz]
        return rcopy(ref, ref, gd_s.at[q, zz], gd_r.at[q, zz], partner, t)

    def pair_send(q):
        for zz in range(nz):
            psend[q][zz] = part[q][(1 - c) * nz + zz].astype(BF16)
        pairs[q].start()

    def line_send(q):
        pairs[q].wait_recv()
        for pz in peers_z:
            zsend[q][pz] = (part[q][c * nz + pz] + pbuf[q][pz].astype(F32)).astype(BF16)
            line(q, pz).start()

    def line_sum(q):
        acc = part[q][me] + pbuf[q][z].astype(F32)
        for pz in peers_z:
            line_got(q, pz).wait_recv()
            acc = acc + zbuf[q][pz].astype(F32)
        tot[q][me] = acc.astype(BF16)
        for pz in peers_z:
            share(q, pz, me).start()
        share_core(q, c, z).start()

    def line_take(q):
        for pz in peers_z:
            share(q, pz, c * nz + pz).wait_recv()
            share_core(q, c, pz).start()

    def direct(q):
        i, r = streams[q]
        if r == 0:
            fetch[8 + i].wait()
            fetch[10 + i].wait()
        for zz in range(nz):
            share_core(q, 1 - c, zz).wait_recv()
        at = pl.ds(r * half, half)
        proj = tot[q][...].astype(F32).reshape(half, tot[q].shape[2])
        mean_out = MEAN_DECAY * mean[i][at, :] + (1.0 - MEAN_DECAY) * proj
        square_out = BETA_SQUARE * square[i][at, :] + (1.0 - BETA_SQUARE) * proj * proj
        mean_new[i][at, :] = mean_out
        square_new[i][at, :] = square_out
        dirs[i][at, :] = (mean_out / jnp.sqrt(square_out)).astype(BF16)

    def norm(i):
        height = bg[i].shape[1]
        group = max(1, 1024 // height)
        sums = jnp.zeros((1, dirs[i].shape[1]), F32)
        for g in range(0, nf, group):
            some = bg[i][g:g + group]
            u = jnp.dot(some.reshape(some.shape[0] * height, rank), dirs[i][...], preferred_element_type=F32)
            sums = sums + jnp.sum(u * u, axis=0, keepdims=True)
        tile = jnp.zeros((8, 128), F32) + jnp.sum(sums, axis=1, keepdims=True)
        tsend[i] = tile
        tbuf[t, i] = tile

    def rest_send(i):
        def parts():
            for b in peers_z:
                for pt in peers_t:
                    @pl.when(pt != b)
                    def _():
                        rest_plane(i, b, t, pt).start()
        when_part(i, t, parts)

        @pl.when(elsewhere)
        def _():
            rest_core(i, f).start()

    def rest_take(i):
        for b in peers_z:
            @pl.when(b != t)
            def _():
                for pt in peers_t:
                    when_part(i, pt, lambda: rest_plane(i, b, pt, pt).wait_recv())
                rest_core(i, b * CORES + c).start()

    def rest_end(i):
        for pt in peers_t:
            rest_core(i, pt * CORES + 1 - c).wait_recv()

    for k in range(len(chunks)):
        basis_in(k)
    for k in range(len(chunks)):
        basis_joined(k)
    fetch[0].wait()
    basis_core(0, other).wait_recv()
    lift(0)
    basis_core(1, other).wait_recv()
    lift(1)
    for u in range(len(units)):
        w_core(u, z, c).start()
    fetch[1].wait()
    basis_core(2, other).wait_recv()
    halve(0, 0)
    lift(2)
    weights_on(NEAR[0])
    halve(1, 0)
    for k in range(1, levels - 1):
        for q in PAIR:
            halve(q, k)
    halve(0, levels - 1)
    lift(3)
    weights_on(NEAR[1])
    halve(1, levels - 1)
    for k in range(levels - 1, 0, -1):
        for q in PAIR:
            double(q, k)
    weights_on(NEAR[2])
    halve(2, 0)
    double(0, 0)
    pair_send(0)
    halve(3, 0)
    double(1, 0)
    pair_send(1)
    for k in range(1, levels - 1):
        for q in (2, 3):
            halve(q, k)
    line_send(0)
    halve(2, levels - 1)
    line_send(1)
    halve(3, levels - 1)
    weights_on(NEAR[3])
    for k in range(levels - 1, 0, -1):
        for q in (2, 3):
            double(q, k)
    weights_on(NEAR[4])
    double(2, 0)
    pair_send(2)
    line_sum(0)
    double(3, 0)
    pair_send(3)
    for i in PAIR:
        rest_send(i)
    line_sum(1)
    line_send(2)
    line_send(3)
    weights_on(NEAR[5])
    line_take(0)
    line_take(1)
    for i in PAIR:
        rest_take(i)
    line_sum(2)
    line_sum(3)
    weights_on(NEAR[6])
    direct(0)
    direct(1)
    for i in PAIR:
        rest_end(i)
    norm(0)
    line_take(2)
    line_take(3)
    weights_on(NEAR[7])
    direct(2)
    direct(3)
    norm(1)
    for pt in peers_t:
        rcopy(tsend, tbuf.at[t], t_s.at[pt], t_r.at[t], f, pt).start()
    weights_on([(s, u) for s in range(3, nz) for u in range(len(units))])

    for pt in peers_t:
        rcopy(tsend, tbuf.at[pt], t_s.at[pt], t_r.at[pt], f, pt).wait_recv()
    summed = tbuf[0]
    for k in range(1, nt):
        summed = summed + tbuf[k]
    totals[...] = summed

    for u in range(len(units)):
        for zb in range(nz):
            w_core(u, zb, 1 - c).wait_recv()
    for k in range(len(chunks)):
        def line_out(k=k):
            for pz in peers_z:
                basis_line(k, pz, f).wait_send()

                @pl.when(pz != t)
                def _():
                    basis_plane(k, pz, t).wait_send()
        when_part(chunks[k][0], t, line_out)
        basis_core(k, lane).wait_send()
    for i in PAIR:
        def rest_out(i=i):
            for b in peers_z:
                for pt in peers_t:
                    @pl.when(pt != b)
                    def _():
                        rest_plane(i, b, t, pt).wait_send()
        when_part(i, t, rest_out)

        @pl.when(elsewhere)
        def _():
            rest_core(i, f).wait_send()
        for b in peers_z:
            @pl.when(b != t)
            def _():
                rest_core(i, b * CORES + c).wait_send()
    for q in range(4):
        for h in PAIR:
            for k in range(levels):
                rs(q, h, k).wait_send()
                ag(q, h, k).wait_send()
        pairs[q].wait_send()
        for pz in peers_z:
            line(q, pz).wait_send()
            share(q, pz, me).wait_send()
        for zz in range(nz):
            share_core(q, c, zz).wait_send()
    for u in range(len(units)):
        for zb in range(nz):
            w_core(u, zb, c).wait_send()

            @pl.when((z >= zb) & (z < nz - 1))
            def _():
                w_up(u, zb).wait_send()

            @pl.when((z <= zb) & (z > 0))
            def _():
                w_dn(u, zb).wait_send()
    for pt in peers_t:
        rcopy(tsend, tbuf.at[t], t_s.at[pt], t_r.at[t], f, pt).wait_send()


def gather_and_reduce(nf, nt, lefts, rights, weights, bases, means, squares):
    rank, nz, tokens = bases[0].shape[1], nf // CORES, rights[0].shape[0]
    half, levels = rank // 2, nt.bit_length() - 1
    seg = half // nf
    heights, widths = [b.shape[0] for b in bases], [r.shape[1] for r in rights]
    units = sum(h // u for h, u in zip(heights, unit_heights(heights, widths)))
    vmem, dma = pl.BlockSpec(memory_space=pltpu.VMEM), pltpu.SemaphoreType.DMA
    hbm = pl.BlockSpec(memory_space=pltpu.HBM)

    def two(shape_of, kind=BF16, make=pltpu.VMEM):
        return [make(shape_of(h, w), kind) for h, w in zip(heights, widths)]

    def four(shape_of, kind=BF16):
        return [pltpu.VMEM(shape_of(w), kind) for w in widths for _ in PAIR]

    def outs(shape_of, kind=BF16):
        return two(shape_of, kind, jax.ShapeDtypeStruct)

    halves = lambda w: (2, tokens // 2, half)
    pieces = lambda w: (nz, seg, w)
    ranked = lambda h, w: (rank, w)
    fetched = (*lefts, *rights, *means, *squares)
    return pl.pallas_call(
        functools.partial(exchange, nf, nt),
        out_shape=(
            *outs(lambda h, w: (nf, h, w)), *outs(lambda h, w: (nf, h, rank)), *outs(ranked),
            *outs(ranked, F32), *outs(ranked, F32), *outs(lambda h, w: (h, w), F32),
            jax.ShapeDtypeStruct((2, 8, 128), F32),
        ),
        in_specs=[hbm] * 12,
        out_specs=(vmem,) * 13,
        scratch_shapes=[
            *[pltpu.VMEM(x.shape, x.dtype) for x in fetched],
            *four(halves), *four(halves), *four(halves, F32), *four(lambda w: (tokens, half)),
            *four(lambda w: (nf, seg, w), F32), *four(pieces), *four(pieces), *four(pieces), *four(pieces),
            *four(lambda w: (nf, seg, w)),
            pltpu.VMEM((2, 8, 128), F32),
            pltpu.VMEM((nt, 2, 8, 128), F32),
            dma((12,)), dma((3, nz)), dma((3, nz)), dma((3,)), dma((3,)),
            dma((3, nz)), dma((3, nt)), dma((2, nz, nt)), dma((2, nz, nt)), dma((2, nf)), dma((2, nf)),
            *[dma((units, nz))] * 5,
            *[dma((4, 2, levels))] * 4,
            dma((4,)), dma((4,)), *[dma((4, nz))] * 6, dma((nt,)), dma((nt,)),
        ],
        compiler_params=pltpu.CompilerParams(
            collective_id=0, has_side_effects=True, vmem_limit_bytes=40 * 1024 * 1024
        ),
        name="exchange",
    )(*[pltpu.with_memory_space_constraint(x, pltpu.HBM)
        for x in (*lefts, *rights, *weights, *bases, *means, *squares)])


def apply(nf, nt, *refs):
    wg, bg, dirs, mean_new, square_new, w32 = (refs[2 * k:2 * k + 2] for k in range(6))
    totals = refs[12]
    outs = [refs[13 + 5 * i:18 + 5 * i] for i in PAIR]
    step, new, copy = (refs[23 + 2 * k:25 + 2 * k] for k in range(3))
    sem, csem = refs[29:]
    f = lax.axis_index("fs")

    def to(k, i):
        src = (step, new, None, mean_new, square_new)[k]
        return pltpu.make_async_copy(src[i], outs[i][k], sem.at[i, k])

    def block(i, g):
        height = w32[i].shape[0]
        return pltpu.make_async_copy(copy[i].at[pl.ds(g * height, height)],
                                     outs[i][2].at[pl.ds(g * height, height)], csem.at[i, g])

    for i in PAIR:
        to(3, i).start()
        to(4, i).start()
    scales = []
    for i in PAIR:
        count = w32[i].shape[0] * nf * w32[i].shape[1] * nt
        scale = LEARN_RATE * lax.rsqrt(totals[i, 0:1, 0:1] / lax.convert_element_type(count, F32) + EPS_RMS)
        scales.append(scale)
        own = scale * jnp.dot(bg[i][f], dirs[i][...], preferred_element_type=F32)
        step[i][...] = own
        new[i][...] = w32[i][...] - own
        to(0, i).start()
        to(1, i).start()
    for i in PAIR:
        height = w32[i].shape[0]
        for g in range(nf):
            update = jnp.dot(bg[i][g], dirs[i][...], preferred_element_type=F32)
            copy[i][pl.ds(g * height, height), :] = (wg[i][g].astype(F32) - scales[i] * update).astype(BF16)
            block(i, g).start()
    for i in PAIR:
        for k in (0, 1, 3, 4):
            to(k, i).wait()
        for g in range(nf):
            block(i, g).wait()


def finish(nf, nt, gathered):
    w32 = gathered[10:12]
    vmem, hbm = pl.BlockSpec(memory_space=pltpu.VMEM), pl.BlockSpec(memory_space=pltpu.HBM)
    out_shape = []
    for i in PAIR:
        copy = jax.ShapeDtypeStruct((nf * w32[i].shape[0], w32[i].shape[1]), BF16)
        like = lambda x: jax.ShapeDtypeStruct(x.shape, F32)
        out_shape += [like(w32[i]), like(w32[i]), copy, like(gathered[6 + i]), like(gathered[8 + i])]
    return pl.pallas_call(
        functools.partial(apply, nf, nt),
        in_specs=[vmem] * 13,
        out_specs=[hbm] * 10,
        out_shape=out_shape,
        scratch_shapes=[
            *[pltpu.VMEM(w.shape, F32) for w in w32], *[pltpu.VMEM(w.shape, F32) for w in w32],
            *[pltpu.VMEM(out_shape[2 + 5 * i].shape, BF16) for i in PAIR],
            pltpu.SemaphoreType.DMA((2, 5)), pltpu.SemaphoreType.DMA((2, nf)),
        ],
        compiler_params=pltpu.CompilerParams(vmem_limit_bytes=12 * 1024 * 1024),
        name="apply",
    )(*gathered)


def per_device(nf, nt, attn_out, out_cot, latent, value_cot, out_weight, value_up_matrix,
               out_basis, value_basis, out_mean, out_square, value_mean, value_square):
    gathered = gather_and_reduce(
        nf, nt, (attn_out, latent), (out_cot, value_cot), (out_weight, value_up_matrix),
        (out_basis, value_basis), (out_mean, value_mean), (out_square, value_square))
    return tuple(finish(nf, nt, gathered))


def solution(mesh):
    both, rows, cols = P("fs", "tp"), P("fs", None), P(None, "tp")
    return jax.shard_map(
        functools.partial(per_device, mesh.shape["fs"], mesh.shape["tp"]),
        mesh=mesh,
        in_specs=(both,) * 6 + (rows,) * 2 + (cols,) * 4,
        out_specs=(both, both, cols, cols, cols) * 2,
        check_vma=False,
    )
```

```python
import functools

import jax
import jax.numpy as jnp
from jax import lax
from jax.experimental import pallas as pl
from jax.experimental.pallas import tpu as pltpu
from jax.sharding import PartitionSpec as P

LEARN_RATE = 0.01
MEAN_DECAY = 0.8
BETA_SQUARE = 0.9
EPS_RMS = 1e-06
MESH = pl.DeviceIdType.MESH
F32, BF16 = jnp.float32, jnp.bfloat16
PAIR = (0, 1)
CORES = 2
NEAR = (((1, 0), (1, 1)), ((1, 2), (1, 3)), ((1, 4), (2, 0)), ((2, 1),), ((2, 2),), ((2, 3),), ((2, 4),))


def rcopy(src, dst, send, recv, fs, tp):
    return pltpu.make_async_remote_copy(
        src_ref=src, dst_ref=dst, send_sem=send, recv_sem=recv,
        device_id=(fs, tp), device_id_type=MESH,
    )


def over_rows(left, right):
    return lax.dot_general(left, right, (((0,), (0,)), ((), ())), preferred_element_type=F32)


def unit_heights(heights, widths):
    least = min(h * w for h, w in zip(heights, widths))
    return [least // w for w in widths]


def parts_of(height, nt):
    return min(nt, height // 16)


def exchange(nf, nt, *refs):
    hbm, rest = refs[:12], refs[12:]
    wg, full, mean_new, square_new, w32 = (rest[2 * k:2 * k + 2] for k in range(5))
    totals, rest = rest[10], rest[11:]
    left, right, mean, square, bg, dirs = (rest[2 * k:2 * k + 2] for k in range(6))
    sbuf, rbuf, kept, lifted, part, psend, pbuf, zsend, zbuf, tot = (rest[12 + 4 * k:16 + 4 * k] for k in range(10))
    (tsend, tbuf, isem, b_s, b_r, bd_s, bd_r, c_s, c_r, e_s, e_r, cd_s, cd_r, w_u, w_d, w_r, wd_s, wd_r,
     rs_s, rs_r, ag_s, ag_r, p_s, p_r, z_s, z_r, g_s, g_r, gd_s, gd_r, t_s, t_r) = rest[52:]

    nz = nf // CORES
    f, t = lax.axis_index("fs"), lax.axis_index("tp")
    z, c = lax.div(f, CORES), lax.rem(f, CORES)
    partner = f + 1 - 2 * c
    rank = bg[0].shape[2]
    half = rank // 2
    tokens = left[0].shape[0]
    peers_t = [lax.rem(t + s, nt) for s in range(1, nt)]
    peers_z = [lax.rem(z + s, nz) for s in range(1, nz)]
    own_column = z == t
    elsewhere = jnp.logical_not(own_column)

    held = (*left, *right, *w32, *[b.at[f] for b in bg], *mean, *square)
    order = (6, 7, 4, 5, 0, 1, 2, 3, 8, 9, 10, 11)
    fetch = [pltpu.make_async_copy(hbm[k], held[k], isem.at[k]) for k in range(12)]
    for k in order:
        fetch[k].start()

    barrier = pltpu.get_barrier_semaphore()
    pl.semaphore_signal(barrier, inc=1, device_id=(partner, t), device_id_type=MESH)
    for pz in peers_z:
        pl.semaphore_signal(barrier, inc=1, device_id=(pz * CORES + c, t), device_id_type=MESH)
    for pt in peers_t:
        pl.semaphore_signal(barrier, inc=1, device_id=(f, pt), device_id_type=MESH)
    pl.semaphore_wait(barrier, 1 + len(peers_z) + len(peers_t))

    def took(ref, sem):
        pltpu.make_async_copy(ref, ref, sem).wait()

    def took_slabs(k_or_i, sem, count, first=0, size=None):
        size = rank if size is None else size
        i = k_or_i
        tall = bg[i].shape[1] // parts_of(bg[i].shape[1], nt)
        took(lifted[0].at[pl.ds(0, count * tall * size // half)], sem)

    lane = t * CORES + c
    other = t * CORES + 1 - c
    chunks = ((0, 0, half), (0, half, half), (1, 0, rank))

    def slab(i, block, column, first=0, size=rank):
        tall = bg[i].shape[1] // parts_of(bg[i].shape[1], nt)
        return bg[i].at[block, pl.ds(pl.multiple_of(column * tall, tall), tall), pl.ds(first, size)]

    def when_part(i, column, then):
        parts = parts_of(bg[i].shape[1], nt)
        if parts == nt:
            then()
        else:
            pl.when(column < parts)(then)

    def basis_line(k, pz, block):
        i, first, size = chunks[k]
        ref = slab(i, block, t, first, size)
        return rcopy(ref, ref, b_s.at[k], b_r.at[k], pz * CORES + c, t)

    def basis_plane(k, b, column):
        i, first, size = chunks[k]
        ref = slab(i, b * CORES + c, column, first, size)
        return rcopy(ref, ref, c_s.at[k], c_r.at[k], f, b)

    def basis_core(k, block):
        i, first, size = chunks[k]
        ref = bg[i].at[block, :, pl.ds(first, size)]
        return rcopy(ref, ref, bd_s.at[k], bd_r.at[k], partner, t)

    def rest_plane(i, b, column, pt):
        ref = slab(i, b * CORES + c, column)
        return rcopy(ref, ref, e_s.at[i, b], e_r.at[i, b], f, pt)

    def rest_core(i, block):
        ref = bg[i].at[block]
        return rcopy(ref, ref, cd_s.at[i], cd_r.at[i], partner, t)

    heights = [w.shape[1] for w in wg]
    tall = unit_heights(heights, [w.shape[2] for w in wg])
    units = [(i, r) for i in PAIR for r in range(0, heights[i], tall[i])]

    def unit(u, zb, core):
        i, r = units[u]
        return wg[i].at[zb * CORES + core, pl.ds(r, tall[i])]

    def w_up(u, zb):
        ref = unit(u, zb, c)
        return rcopy(ref, ref, w_u.at[units[u][0]], w_r.at[u, zb], f + CORES, t)

    def w_dn(u, zb):
        ref = unit(u, zb, c)
        return rcopy(ref, ref, w_d.at[units[u][0]], w_r.at[u, zb], f - CORES, t)

    def w_core(u, zb, core):
        ref = unit(u, zb, core)
        return rcopy(ref, ref, wd_s.at[units[u][0]], wd_r.at[units[u][0]], partner, t)

    def weights_on(events):
        for s, u in events:
            if s > nz - 1:
                continue

            @pl.when(z >= s)
            def _():
                w_up(u, z - s).wait_recv()

                @pl.when(z < nz - 1)
                def _():
                    w_up(u, z - s).start()
                w_core(u, z - s, c).start()

            @pl.when(z + s <= nz - 1)
            def _():
                w_dn(u, z + s).wait_recv()

                @pl.when(z > 0)
                def _():
                    w_dn(u, z + s).start()
                w_core(u, z + s, c).start()

    fetch[6].wait()
    fetch[7].wait()
    for k in range(len(chunks)):
        def to_line(k=k):
            for pz in [lax.rem(z + s, nz) for s in range(nz // 2, nz)] + [lax.rem(z + s, nz) for s in range(1, nz // 2)]:
                basis_line(k, pz, f).start()
        when_part(chunks[k][0], t, to_line)

    @pl.when(own_column)
    def _():
        for k in range(len(chunks)):
            basis_core(k, lane).start()
    for i in PAIR:
        fetch[4 + i].wait()
        wg[i][f] = w32[i][...].astype(BF16)
    for u in range(len(units)):
        @pl.when(z < nz - 1)
        def _():
            w_up(u, z).start()

        @pl.when(z > 0)
        def _():
            w_dn(u, z).start()

    levels = nt.bit_length() - 1
    sizes = [tokens // 2 >> k for k in range(levels + 1)]
    offs = [sizes[0] - s for s in sizes]
    masks = [[1 << k for k in range(levels)], [1 << k for k in reversed(range(levels))]]
    bits = [[lax.rem(lax.div(t, m), 2) for m in masks[h]] for h in PAIR]
    mates = [[t + m * (1 - 2 * b) for m, b in zip(masks[h], bits[h])] for h in PAIR]
    bases = []
    for h in PAIR:
        at = [h * sizes[0]]
        for k in range(levels):
            at.append(at[-1] + bits[h][k] * sizes[k + 1])
        bases.append(at)
    streams = tuple((i, r) for i in PAIR for r in PAIR)

    def rows(start, size):
        return pl.ds(pl.multiple_of(start, 16), size)

    def away(h, k):
        return rows(bases[h][k] + (1 - bits[h][k]) * sizes[k + 1], sizes[k + 1])

    def rs(q, h, k):
        at = pl.ds(offs[k], sizes[k + 1])
        return rcopy(sbuf[q].at[h, at], rbuf[q].at[h, at], rs_s.at[q], rs_r.at[q, k], f, mates[h][k])

    def ag(q, h, k):
        ref = lifted[q].at[rows(bases[h][k + 1], sizes[k + 1])]
        return rcopy(ref, ref, ag_s.at[q], ag_r.at[q, k], f, mates[h][k])

    def senders(i, then):
        parts = parts_of(bg[i].shape[1], nt)
        if parts == nt:
            then(nt - 1)
        else:
            pl.when(t < parts)(lambda: then(parts - 1))
            pl.when(t >= parts)(lambda: then(parts))

    def basis_in(k):
        i, first, size = chunks[k]

        def from_line():
            took_slabs(i, b_r.at[k], nz - 1, size=size)
            for b in peers_z:
                @pl.when(b != t)
                def _():
                    basis_plane(k, b, t).start()

        when_part(i, t, from_line)

    def basis_joined(k):
        i, first, size = chunks[k]

        @pl.when(elsewhere)
        def _():
            senders(i, lambda n: took_slabs(i, c_r.at[k], n, size=size))
            basis_core(k, lane).start()

    def lift(q):
        i, r = streams[q]
        two = bg[i][pl.ds(t * CORES, CORES), :, r * half:(r + 1) * half]
        factor = two.reshape(two.shape[0] * two.shape[1], half)
        for h in PAIR:
            sbuf[q][h, pl.ds(0, sizes[1])] = jnp.dot(
                left[i][away(h, 0), :], factor, preferred_element_type=F32).astype(BF16)
            rs(q, h, 0).start()
        for h in PAIR:
            kept[q][h, pl.ds(0, sizes[1])] = jnp.dot(
                left[i][rows(bases[h][1], sizes[1]), :], factor, preferred_element_type=F32)

    def contract(q, at, first=False):
        i = streams[q][0]
        got = over_rows(lifted[q][at, :], right[i][at, :]).reshape(part[q].shape)
        if first:
            part[q][...] = got
        else:
            part[q][...] += got

    def halve(q, k):
        took(rbuf[q].at[:, pl.ds(offs[k], sizes[k + 1])], rs_r.at[q, k])
        for h in PAIR:
            if k + 1 < levels:
                small = sizes[k + 2]
                for b, mine in ((1 - bits[h][k + 1], False), (bits[h][k + 1], True)):
                    at = rows(offs[k] + b * small, small)
                    both = kept[q][h, at] + rbuf[q][h, at].astype(F32)
                    to = pl.ds(offs[k + 1], small)
                    if mine:
                        kept[q][h, to] = both
                    else:
                        sbuf[q][h, to] = both.astype(BF16)
                        rs(q, h, k + 1).start()
            else:
                at = pl.ds(offs[k], sizes[k + 1])
                lifted[q][rows(bases[h][k + 1], sizes[k + 1]), :] = (
                    kept[q][h, at] + rbuf[q][h, at].astype(F32)).astype(BF16)
                ag(q, h, k).start()
        if k + 1 == levels:
            i, r = streams[q]
            if r == 0:
                fetch[2 + i].wait()
            for h in PAIR:
                contract(q, rows(bases[h][levels], sizes[levels]), h == 0)

    def double(q, k):
        took(lifted[q].at[pl.ds(0, 2 * sizes[k + 1])], ag_r.at[q, k])
        if k > 0:
            for h in PAIR:
                ag(q, h, k - 1).start()
        for h in PAIR:
            contract(q, away(h, k))

    pairs = [rcopy(psend[q], pbuf[q], p_s.at[q], p_r.at[q], partner, t) for q in range(4)]
    me = c * nz + z

    chained = (0, 1)

    def line(q, pz):
        return rcopy(zsend[q].at[pz], zbuf[q].at[z], z_s.at[q], z_r.at[q, 0], pz * CORES + c, t)

    def hop(q, zz, up, slot):
        return rcopy(zsend[q].at[zz], zbuf[q].at[slot], z_s.at[q], z_r.at[q, 0 if up else 1],
                     f + (CORES if up else -CORES), t)

    def line_step(q, k):
        for at, up in ((k, True), (nz - 1 - k, False)):
            @pl.when(z == at)
            def _():
                if k > 0:
                    took(zbuf[q].at[pl.ds(0, nz - k)], z_r.at[q, 0 if up else 1])
                for zz in (range(at + 1, nz) if up else range(at)):
                    sums = part[q][c * nz + zz] + pbuf[q][zz].astype(F32)
                    if k > 0:
                        sums = sums + zbuf[q][zz].astype(F32)
                    zsend[q][zz] = sums.astype(BF16)
                    beside = at + 1 if up else at - 1
                    hop(q, zz, up, nz if zz == beside and not up else zz).start()

    def share(q, pz, at):
        ref = tot[q].at[at]
        return rcopy(ref, ref, g_s.at[q], g_r.at[q], pz * CORES + c, t)

    def share_core(q):
        ref = tot[q].at[pl.ds(c * nz, nz)]
        return rcopy(ref, ref, gd_s.at[q], gd_r.at[q], partner, t)

    def pair_send(q):
        for zz in range(nz):
            psend[q][zz] = part[q][(1 - c) * nz + zz].astype(BF16)
        pairs[q].start()

    def line_send(q):
        pairs[q].wait_recv()
        if q in chained:
            line_step(q, 0)
            return
        for pz in peers_z:
            zsend[q][pz] = (part[q][c * nz + pz] + pbuf[q][pz].astype(F32)).astype(BF16)
            line(q, pz).start()

    def line_sum(q):
        acc = part[q][me] + pbuf[q][z].astype(F32)
        if q in chained:
            for at in range(nz):
                @pl.when(z == at)
                def _():
                    sums = acc
                    if at > 0:
                        if at == nz - 1:
                            took(zbuf[q].at[pl.ds(0, 1)], z_r.at[q, 0])
                        sums = sums + zbuf[q][at].astype(F32)
                    if at < nz - 1:
                        if at == 0:
                            took(zbuf[q].at[pl.ds(0, 1)], z_r.at[q, 1])
                        sums = sums + zbuf[q][nz].astype(F32)
                    tot[q][at + c * nz] = sums.astype(BF16)
        else:
            took(zbuf[q].at[pl.ds(0, nz - 1)], z_r.at[q, 0])
            for pz in peers_z:
                acc = acc + zbuf[q][pz].astype(F32)
            tot[q][me] = acc.astype(BF16)
        for pz in peers_z:
            share(q, pz, me).start()

    def line_take(q):
        took(tot[q].at[pl.ds(0, nz - 1)], g_r.at[q])
        share_core(q).start()

    def direct(q):
        i, r = streams[q]
        if r == 0:
            fetch[8 + i].wait()
            fetch[10 + i].wait()
        share_core(q).wait_recv()
        at = pl.ds(r * half, half)
        proj = tot[q][...].astype(F32).reshape(half, tot[q].shape[2])
        mean_out = MEAN_DECAY * mean[i][at, :] + (1.0 - MEAN_DECAY) * proj
        square_out = BETA_SQUARE * square[i][at, :] + (1.0 - BETA_SQUARE) * proj * proj
        mean_new[i][at, :] = mean_out
        square_new[i][at, :] = square_out
        dirs[i][at, :] = (mean_out / jnp.sqrt(square_out)).astype(BF16)

    def norm(i):
        height = bg[i].shape[1]
        group = max(1, 1024 // height)
        sums = jnp.zeros((1, dirs[i].shape[1]), F32)
        for g in range(0, nf, group):
            some = bg[i][g:g + group]
            u = jnp.dot(some.reshape(some.shape[0] * height, rank), dirs[i][...], preferred_element_type=F32)
            full[i][g * height:(g + some.shape[0]) * height, :] = u
            sums = sums + jnp.sum(u * u, axis=0, keepdims=True)
        tile = jnp.zeros((8, 128), F32) + jnp.sum(sums, axis=1, keepdims=True)
        tsend[i] = tile
        tbuf[t, i] = tile

    def rest_send(i):
        def parts():
            for b in peers_z:
                for pt in peers_t:
                    @pl.when(pt != b)
                    def _():
                        rest_plane(i, b, t, pt).start()
        when_part(i, t, parts)

        @pl.when(elsewhere)
        def _():
            rest_core(i, f).start()

    def rest_take(i):
        for b in peers_z:
            @pl.when(b != t)
            def _():
                senders(i, lambda n: took_slabs(i, e_r.at[i, b], n))
                rest_core(i, b * CORES + c).start()

    def rest_end(i):
        took(bg[i].at[pl.ds(0, nz - 1)], cd_r.at[i])

    def basis_gone():
        for k, (i, first, size) in enumerate(chunks):
            def line_out(k=k, i=i, size=size):
                took_slabs(i, b_s.at[k], nz - 1, size=size)
                pl.when(elsewhere)(lambda: took_slabs(i, c_s.at[k], nz - 2, size=size))
                pl.when(own_column)(lambda: took_slabs(i, c_s.at[k], nz - 1, size=size))
            when_part(i, t, line_out)
            basis_core(k, lane).wait_send()

    def rest_gone():
        for i in PAIR:
            def rest_out(i=i):
                for b in peers_z:
                    pl.when(b == t)(lambda: took_slabs(i, e_s.at[i, b], nt - 1))
                    pl.when(b != t)(lambda: took_slabs(i, e_s.at[i, b], nt - 2))
            when_part(i, t, rest_out)
            took(bg[i].at[pl.ds(0, nz - 1)], cd_s.at[i])

    def tokens_gone(q):
        sent = 2 * sum(sizes[1:])
        took(lifted[q].at[pl.ds(0, sent)], rs_s.at[q])
        took(lifted[q].at[pl.ds(0, sent)], ag_s.at[q])

    def line_gone(q):
        pairs[q].wait_send()
        took(zsend[q].at[pl.ds(0, nz - 1)], z_s.at[q])
        took(tot[q].at[pl.ds(0, nz - 1)], g_s.at[q])
        share_core(q).wait_send()

    def weights_gone():
        for i in PAIR:
            took(wg[i].at[pl.ds(0, nz)], wd_s.at[i])
            for at in range(nz):
                @pl.when(z == at)
                def _():
                    if at < nz - 1:
                        took(wg[i].at[pl.ds(0, at + 1)], w_u.at[i])
                    if at > 0:
                        took(wg[i].at[pl.ds(0, nz - at)], w_d.at[i])

    for k in range(len(chunks)):
        basis_in(k)
    for k in range(len(chunks)):
        basis_joined(k)
    fetch[0].wait()
    basis_core(0, other).wait_recv()
    lift(0)
    basis_core(1, other).wait_recv()
    lift(1)
    for u in range(len(units)):
        w_core(u, z, c).start()
    fetch[1].wait()
    basis_core(2, other).wait_recv()
    halve(0, 0)
    lift(2)
    weights_on(NEAR[0])
    halve(1, 0)
    for k in range(1, levels - 1):
        for q in PAIR:
            halve(q, k)
    halve(0, levels - 1)
    lift(3)
    weights_on(NEAR[1])
    halve(1, levels - 1)
    for k in range(levels - 1, 0, -1):
        for q in PAIR:
            double(q, k)
    weights_on(NEAR[2])
    halve(2, 0)
    double(0, 0)
    pair_send(0)
    halve(3, 0)
    double(1, 0)
    pair_send(1)
    for k in range(1, levels - 1):
        for q in (2, 3):
            halve(q, k)
    line_send(0)
    halve(2, levels - 1)
    line_send(1)
    halve(3, levels - 1)
    weights_on(NEAR[3])
    for k in range(levels - 1, 0, -1):
        for q in (2, 3):
            double(q, k)
    line_step(0, 1)
    line_step(1, 1)
    weights_on(NEAR[4])
    double(2, 0)
    pair_send(2)
    for k in range(2, nz - 1):
        line_step(0, k)
        line_step(1, k)
    double(3, 0)
    pair_send(3)
    line_send(2)
    line_send(3)
    line_sum(0)
    line_sum(1)
    for i in PAIR:
        rest_send(i)
    weights_on(NEAR[5])
    basis_gone()
    tokens_gone(0)
    tokens_gone(1)
    line_sum(2)
    line_sum(3)
    weights_on(NEAR[6])
    line_take(0)
    line_take(1)
    for i in PAIR:
        rest_take(i)
    direct(0)
    direct(1)
    for i in PAIR:
        rest_end(i)
    norm(0)
    line_take(2)
    line_take(3)
    direct(2)
    direct(3)
    norm(1)
    for pt in peers_t:
        rcopy(tsend, tbuf.at[t], t_s.at[0], t_r.at[0], f, pt).start()
    rest_gone()
    tokens_gone(2)
    tokens_gone(3)
    for q in range(4):
        line_gone(q)
    weights_on([(s, u) for s in range(3, nz) for u in range(len(units))])
    took(tbuf.at[pl.ds(0, nt - 1)], t_r.at[0])
    summed = tbuf[0]
    for k in range(1, nt):
        summed = summed + tbuf[k]
    totals[...] = summed
    for i in PAIR:
        took(wg[i].at[pl.ds(0, nz)], wd_r.at[i])
    weights_gone()
    took(tbuf.at[pl.ds(0, nt - 1)], t_s.at[0])


def gather_and_reduce(nf, nt, lefts, rights, weights, bases, means, squares):
    rank, nz, tokens = bases[0].shape[1], nf // CORES, rights[0].shape[0]
    half, levels = rank // 2, nt.bit_length() - 1
    seg = half // nf
    heights, widths = [b.shape[0] for b in bases], [r.shape[1] for r in rights]
    units = sum(h // u for h, u in zip(heights, unit_heights(heights, widths)))
    vmem, dma = pl.BlockSpec(memory_space=pltpu.VMEM), pltpu.SemaphoreType.DMA
    hbm = pl.BlockSpec(memory_space=pltpu.HBM)

    def two(shape_of, kind=BF16, make=pltpu.VMEM):
        return [make(shape_of(h, w), kind) for h, w in zip(heights, widths)]

    def four(shape_of, kind=BF16):
        return [pltpu.VMEM(shape_of(w), kind) for w in widths for _ in PAIR]

    def outs(shape_of, kind=BF16):
        return two(shape_of, kind, jax.ShapeDtypeStruct)

    halves = lambda w: (2, tokens // 2, half)
    pieces = lambda w: (nz, seg, w)
    ranked = lambda h, w: (rank, w)
    fetched = (*lefts, *rights, *means, *squares)
    return pl.pallas_call(
        functools.partial(exchange, nf, nt),
        out_shape=(
            *outs(lambda h, w: (nf, h, w)), *outs(lambda h, w: (nf * h, w), F32),
            *outs(ranked, F32), *outs(ranked, F32), *outs(lambda h, w: (h, w), F32),
            jax.ShapeDtypeStruct((2, 8, 128), F32),
        ),
        in_specs=[hbm] * 12,
        out_specs=(vmem,) * 11,
        scratch_shapes=[
            *[pltpu.VMEM(x.shape, x.dtype) for x in fetched], *two(lambda h, w: (nf, h, rank)), *two(ranked),
            *four(halves), *four(halves), *four(halves, F32), *four(lambda w: (tokens, half)),
            *four(lambda w: (nf, seg, w), F32), *four(pieces), *four(pieces), *four(pieces),
            *four(lambda w: (nz + 1, seg, w)),
            *four(lambda w: (nf, seg, w)),
            pltpu.VMEM((2, 8, 128), F32),
            pltpu.VMEM((nt, 2, 8, 128), F32),
            dma((12,)), *[dma((3,))] * 6, *[dma((2, nz))] * 2, *[dma((2,))] * 2, dma((2,)), dma((2,)), dma((units, nz)), dma((2,)), dma((2,)),
            dma((4,)), dma((4, levels)), dma((4,)), dma((4, levels)), dma((4,)), dma((4,)), dma((4,)), dma((4, 2)),
            *[dma((4,))] * 4, dma((1,)), dma((1,)),
        ],
        compiler_params=pltpu.CompilerParams(
            collective_id=0, has_side_effects=True, vmem_limit_bytes=34 * 1024 * 1024
        ),
        name="exchange",
    )(*[pltpu.with_memory_space_constraint(x, pltpu.HBM)
        for x in (*lefts, *rights, *weights, *bases, *means, *squares)])


def apply(nf, nt, *refs):
    wg, full, mean_new, square_new, w32 = (refs[2 * k:2 * k + 2] for k in range(5))
    totals = refs[10]
    outs = [refs[11 + 5 * i:16 + 5 * i] for i in PAIR]
    step, new, copy = (refs[21 + 2 * k:23 + 2 * k] for k in range(3))
    sem, csem = refs[27:]
    f = lax.axis_index("fs")

    def to(k, i):
        src = (step, new, None, mean_new, square_new)[k]
        return pltpu.make_async_copy(src[i], outs[i][k], sem.at[i, k])

    def block(i, g):
        height = w32[i].shape[0]
        return pltpu.make_async_copy(copy[i].at[pl.ds(g * height, height)],
                                     outs[i][2].at[pl.ds(g * height, height)], csem.at[i, g])

    for i in PAIR:
        to(3, i).start()
        to(4, i).start()
    scales = []
    for i in PAIR:
        count = w32[i].shape[0] * nf * w32[i].shape[1] * nt
        scale = LEARN_RATE * lax.rsqrt(totals[i, 0:1, 0:1] / lax.convert_element_type(count, F32) + EPS_RMS)
        scales.append(scale)
        height = w32[i].shape[0]
        own = scale * full[i][pl.ds(pl.multiple_of(f * height, height), height), :]
        step[i][...] = own
        new[i][...] = w32[i][...] - own
        to(0, i).start()
        to(1, i).start()
    for i in PAIR:
        height = w32[i].shape[0]
        for g in range(nf):
            at = pl.ds(g * height, height)
            copy[i][at, :] = (wg[i][g].astype(F32) - scales[i] * full[i][at, :]).astype(BF16)
            block(i, g).start()
    for i in PAIR:
        for k in (0, 1, 3, 4):
            to(k, i).wait()
        for g in range(nf):
            block(i, g).wait()


def finish(nf, nt, gathered):
    w32 = gathered[8:10]
    vmem, hbm = pl.BlockSpec(memory_space=pltpu.VMEM), pl.BlockSpec(memory_space=pltpu.HBM)
    out_shape = []
    for i in PAIR:
        copy = jax.ShapeDtypeStruct((nf * w32[i].shape[0], w32[i].shape[1]), BF16)
        like = lambda x: jax.ShapeDtypeStruct(x.shape, F32)
        out_shape += [like(w32[i]), like(w32[i]), copy, like(gathered[4 + i]), like(gathered[6 + i])]
    return pl.pallas_call(
        functools.partial(apply, nf, nt),
        in_specs=[vmem] * 11,
        out_specs=[hbm] * 10,
        out_shape=out_shape,
        scratch_shapes=[
            *[pltpu.VMEM(w.shape, F32) for w in w32], *[pltpu.VMEM(w.shape, F32) for w in w32],
            *[pltpu.VMEM(out_shape[2 + 5 * i].shape, BF16) for i in PAIR],
            pltpu.SemaphoreType.DMA((2, 5)), pltpu.SemaphoreType.DMA((2, nf)),
        ],
        compiler_params=pltpu.CompilerParams(vmem_limit_bytes=12 * 1024 * 1024),
        name="apply",
    )(*gathered)


def per_device(nf, nt, attn_out, out_cot, latent, value_cot, out_weight, value_up_matrix,
               out_basis, value_basis, out_mean, out_square, value_mean, value_square):
    gathered = gather_and_reduce(
        nf, nt, (attn_out, latent), (out_cot, value_cot), (out_weight, value_up_matrix),
        (out_basis, value_basis), (out_mean, value_mean), (out_square, value_square))
    return tuple(finish(nf, nt, gathered))


def solution(mesh):
    both, rows, cols = P("fs", "tp"), P("fs", None), P(None, "tp")
    return jax.shard_map(
        functools.partial(per_device, mesh.shape["fs"], mesh.shape["tp"]),
        mesh=mesh,
        in_specs=(both,) * 6 + (rows,) * 2 + (cols,) * 4,
        out_specs=(both, both, cols, cols, cols) * 2,
        check_vma=False,
    )
```

```python
import functools

import jax
import jax.numpy as jnp
from jax import lax
from jax.experimental import pallas as pl
from jax.experimental.pallas import tpu as pltpu
from jax.sharding import PartitionSpec as P

LEARN_RATE = 0.01
MEAN_DECAY = 0.8
BETA_SQUARE = 0.9
EPS_RMS = 1e-06
MESH = pl.DeviceIdType.MESH
F32, BF16 = jnp.float32, jnp.bfloat16
PAIR = (0, 1)
CORES = 2
NEAR = (((1, 0), (1, 1)), ((1, 2), (1, 3)), ((1, 4), (2, 0)), ((2, 1),), ((2, 2),), (), ((2, 3), (2, 4)))


def rcopy(src, dst, send, recv, fs, tp):
    return pltpu.make_async_remote_copy(
        src_ref=src, dst_ref=dst, send_sem=send, recv_sem=recv,
        device_id=(fs, tp), device_id_type=MESH,
    )


def over_rows(left, right):
    return lax.dot_general(left, right, (((0,), (0,)), ((), ())), preferred_element_type=F32)


def unit_heights(heights, widths):
    least = min(h * w for h, w in zip(heights, widths))
    return [least // w for w in widths]


def parts_of(height, nt):
    return min(nt, height // 16)


def exchange(nf, nt, *refs):
    hbm, rest = refs[:12], refs[12:]
    wg, full, mean_new, square_new, w32 = (rest[2 * k:2 * k + 2] for k in range(5))
    totals, rest = rest[10], rest[11:]
    left, right, mean, square, bg, dirs = (rest[2 * k:2 * k + 2] for k in range(6))
    sbuf, rbuf, kept, lifted, part, psend, pbuf, zsend, zbuf, tot = (rest[12 + 4 * k:16 + 4 * k] for k in range(10))
    (tsend, tbuf, isem, b_s, b_r, bd_s, bd_r, c_s, c_r, e_s, e_r, cd_s, cd_r, w_u, w_d, w_r, wd_s, wd_r,
     rs_s, rs_r, ag_s, ag_r, p_s, p_r, z_s, z_r, g_s, g_r, gd_s, gd_r, t_s, t_r) = rest[52:]

    nz = nf // CORES
    f, t = lax.axis_index("fs"), lax.axis_index("tp")
    z, c = lax.div(f, CORES), lax.rem(f, CORES)
    partner = f + 1 - 2 * c
    rank = bg[0].shape[2]
    half = rank // 2
    tokens = left[0].shape[0]
    peers_t = [lax.rem(t + s, nt) for s in range(1, nt)]
    peers_z = [lax.rem(z + s, nz) for s in range(1, nz)]
    own_column = z == t
    elsewhere = jnp.logical_not(own_column)

    held = (*left, *right, *w32, *[b.at[f] for b in bg], *mean, *square)
    order = (6, 7, 4, 5, 0, 1, 2, 3, 8, 9, 10, 11)
    fetch = [pltpu.make_async_copy(hbm[k], held[k], isem.at[k]) for k in range(12)]
    for k in order:
        fetch[k].start()

    barrier = pltpu.get_barrier_semaphore()
    pl.semaphore_signal(barrier, inc=1, device_id=(partner, t), device_id_type=MESH)
    for pz in peers_z:
        pl.semaphore_signal(barrier, inc=1, device_id=(pz * CORES + c, t), device_id_type=MESH)
    for pt in peers_t:
        pl.semaphore_signal(barrier, inc=1, device_id=(f, pt), device_id_type=MESH)
    pl.semaphore_wait(barrier, 1 + len(peers_z) + len(peers_t))

    def took(ref, sem):
        pltpu.make_async_copy(ref, ref, sem).wait()

    def took_slabs(k_or_i, sem, count, first=0, size=None):
        size = rank if size is None else size
        i = k_or_i
        tall = bg[i].shape[1] // parts_of(bg[i].shape[1], nt)
        took(lifted[0].at[pl.ds(0, count * tall * size // half)], sem)

    lane = t * CORES + c
    other = t * CORES + 1 - c
    chunks = ((0, 0, half), (0, half, half), (1, 0, rank))

    def slab(i, block, column, first=0, size=rank):
        tall = bg[i].shape[1] // parts_of(bg[i].shape[1], nt)
        return bg[i].at[block, pl.ds(pl.multiple_of(column * tall, tall), tall), pl.ds(first, size)]

    def when_part(i, column, then):
        parts = parts_of(bg[i].shape[1], nt)
        if parts == nt:
            then()
        else:
            pl.when(column < parts)(then)

    def basis_line(k, pz, block):
        i, first, size = chunks[k]
        ref = slab(i, block, t, first, size)
        return rcopy(ref, ref, b_s.at[k], b_r.at[k], pz * CORES + c, t)

    def basis_plane(k, b, column):
        i, first, size = chunks[k]
        ref = slab(i, b * CORES + c, column, first, size)
        return rcopy(ref, ref, c_s.at[k], c_r.at[k], f, b)

    def basis_core(k, block):
        i, first, size = chunks[k]
        ref = bg[i].at[block, :, pl.ds(first, size)]
        return rcopy(ref, ref, bd_s.at[k], bd_r.at[k], partner, t)

    def rest_plane(i, b, column, pt):
        ref = slab(i, b * CORES + c, column)
        return rcopy(ref, ref, e_s.at[i, b], e_r.at[i, b], f, pt)

    def rest_core(i, block):
        ref = bg[i].at[block]
        return rcopy(ref, ref, cd_s.at[i], cd_r.at[i], partner, t)

    heights = [w.shape[1] for w in wg]
    tall = unit_heights(heights, [w.shape[2] for w in wg])
    units = [(i, r) for i in PAIR for r in range(0, heights[i], tall[i])]

    def unit(u, zb, core):
        i, r = units[u]
        return wg[i].at[zb * CORES + core, pl.ds(r, tall[i])]

    def w_up(u, zb):
        ref = unit(u, zb, c)
        return rcopy(ref, ref, w_u.at[units[u][0]], w_r.at[u, zb], f + CORES, t)

    def w_dn(u, zb):
        ref = unit(u, zb, c)
        return rcopy(ref, ref, w_d.at[units[u][0]], w_r.at[u, zb], f - CORES, t)

    def w_core(u, zb, core):
        ref = unit(u, zb, core)
        return rcopy(ref, ref, wd_s.at[units[u][0]], wd_r.at[units[u][0]], partner, t)

    def weights_on(events):
        for s, u in events:
            if s > nz - 1:
                continue

            @pl.when(z >= s)
            def _():
                w_up(u, z - s).wait_recv()

                @pl.when(z < nz - 1)
                def _():
                    w_up(u, z - s).start()
                w_core(u, z - s, c).start()

            @pl.when(z + s <= nz - 1)
            def _():
                w_dn(u, z + s).wait_recv()

                @pl.when(z > 0)
                def _():
                    w_dn(u, z + s).start()
                w_core(u, z + s, c).start()

    fetch[6].wait()
    fetch[7].wait()
    for k in range(len(chunks)):
        def to_line(k=k):
            for pz in [lax.rem(z + s, nz) for s in range(nz // 2, nz)] + [lax.rem(z + s, nz) for s in range(1, nz // 2)]:
                basis_line(k, pz, f).start()
        when_part(chunks[k][0], t, to_line)

    @pl.when(own_column)
    def _():
        for k in range(len(chunks)):
            basis_core(k, lane).start()
    for i in PAIR:
        fetch[4 + i].wait()
        wg[i][f] = w32[i][...].astype(BF16)
    for u in range(len(units)):
        @pl.when(z < nz - 1)
        def _():
            w_up(u, z).start()

        @pl.when(z > 0)
        def _():
            w_dn(u, z).start()

    levels = nt.bit_length() - 1
    sizes = [tokens // 2 >> k for k in range(levels + 1)]
    offs = [sizes[0] - s for s in sizes]
    masks = [[1 << k for k in range(levels)], [1 << k for k in reversed(range(levels))]]
    bits = [[lax.rem(lax.div(t, m), 2) for m in masks[h]] for h in PAIR]
    mates = [[t + m * (1 - 2 * b) for m, b in zip(masks[h], bits[h])] for h in PAIR]
    bases = []
    for h in PAIR:
        at = [h * sizes[0]]
        for k in range(levels):
            at.append(at[-1] + bits[h][k] * sizes[k + 1])
        bases.append(at)
    streams = tuple((i, r) for i in PAIR for r in PAIR)

    def rows(start, size):
        return pl.ds(pl.multiple_of(start, 16), size)

    def away(h, k):
        return rows(bases[h][k] + (1 - bits[h][k]) * sizes[k + 1], sizes[k + 1])

    def rs(q, h, k):
        at = pl.ds(offs[k], sizes[k + 1])
        return rcopy(sbuf[q].at[h, at], rbuf[q].at[h, at], rs_s.at[q], rs_r.at[q, k], f, mates[h][k])

    def ag(q, h, k):
        ref = lifted[q].at[rows(bases[h][k + 1], sizes[k + 1])]
        return rcopy(ref, ref, ag_s.at[q], ag_r.at[q, k], f, mates[h][k])

    def senders(i, then):
        parts = parts_of(bg[i].shape[1], nt)
        if parts == nt:
            then(nt - 1)
        else:
            pl.when(t < parts)(lambda: then(parts - 1))
            pl.when(t >= parts)(lambda: then(parts))

    def basis_in(k):
        i, first, size = chunks[k]

        def from_line():
            took_slabs(i, b_r.at[k], nz - 1, size=size)
            for b in peers_z:
                @pl.when(b != t)
                def _():
                    basis_plane(k, b, t).start()

        when_part(i, t, from_line)

    def basis_joined(k):
        i, first, size = chunks[k]

        @pl.when(elsewhere)
        def _():
            senders(i, lambda n: took_slabs(i, c_r.at[k], n, size=size))
            basis_core(k, lane).start()

    def lift(q):
        i, r = streams[q]
        two = bg[i][pl.ds(t * CORES, CORES), :, r * half:(r + 1) * half]
        factor = two.reshape(two.shape[0] * two.shape[1], half)
        for h in PAIR:
            sbuf[q][h, pl.ds(0, sizes[1])] = jnp.dot(
                left[i][away(h, 0), :], factor, preferred_element_type=F32).astype(BF16)
            rs(q, h, 0).start()
        for h in PAIR:
            kept[q][h, pl.ds(0, sizes[1])] = jnp.dot(
                left[i][rows(bases[h][1], sizes[1]), :], factor, preferred_element_type=F32)

    def contract(q, at, first=False):
        i = streams[q][0]
        got = over_rows(lifted[q][at, :], right[i][at, :]).reshape(part[q].shape)
        if first:
            part[q][...] = got
        else:
            part[q][...] += got

    def halve(q, k):
        took(rbuf[q].at[:, pl.ds(offs[k], sizes[k + 1])], rs_r.at[q, k])
        for h in PAIR:
            if k + 1 < levels:
                small = sizes[k + 2]
                for b, mine in ((1 - bits[h][k + 1], False), (bits[h][k + 1], True)):
                    at = rows(offs[k] + b * small, small)
                    both = kept[q][h, at] + rbuf[q][h, at].astype(F32)
                    to = pl.ds(offs[k + 1], small)
                    if mine:
                        kept[q][h, to] = both
                    else:
                        sbuf[q][h, to] = both.astype(BF16)
                        rs(q, h, k + 1).start()
            else:
                at = pl.ds(offs[k], sizes[k + 1])
                lifted[q][rows(bases[h][k + 1], sizes[k + 1]), :] = (
                    kept[q][h, at] + rbuf[q][h, at].astype(F32)).astype(BF16)
                ag(q, h, k).start()
        if k + 1 == levels:
            i, r = streams[q]
            if r == 0:
                fetch[2 + i].wait()
            for h in PAIR:
                contract(q, rows(bases[h][levels], sizes[levels]), h == 0)

    def double(q, k):
        took(lifted[q].at[pl.ds(0, 2 * sizes[k + 1])], ag_r.at[q, k])
        if k > 0:
            for h in PAIR:
                ag(q, h, k - 1).start()
        for h in PAIR:
            contract(q, away(h, k))

    pairs = [rcopy(psend[q], pbuf[q], p_s.at[q], p_r.at[q], partner, t) for q in range(4)]
    me = c * nz + z

    chained = (0, 1)

    def line(q, pz):
        return rcopy(zsend[q].at[pz], zbuf[q].at[z], z_s.at[q], z_r.at[q, 0], pz * CORES + c, t)

    def hop(q, zz, up, slot):
        return rcopy(zsend[q].at[zz], zbuf[q].at[slot], z_s.at[q], z_r.at[q, 0 if up else 1],
                     f + (CORES if up else -CORES), t)

    def line_step(q, k):
        for at, up in ((k, True), (nz - 1 - k, False)):
            @pl.when(z == at)
            def _():
                if k > 0:
                    took(zbuf[q].at[pl.ds(0, nz - k)], z_r.at[q, 0 if up else 1])
                for zz in (range(at + 1, nz) if up else range(at)):
                    sums = part[q][c * nz + zz] + pbuf[q][zz].astype(F32)
                    if k > 0:
                        sums = sums + zbuf[q][zz].astype(F32)
                    zsend[q][zz] = sums.astype(BF16)
                    beside = at + 1 if up else at - 1
                    hop(q, zz, up, nz if zz == beside and not up else zz).start()

    def share(q, pz, at):
        ref = tot[q].at[at]
        return rcopy(ref, ref, g_s.at[q], g_r.at[q], pz * CORES + c, t)

    def share_core(q):
        ref = tot[q].at[pl.ds(c * nz, nz)]
        return rcopy(ref, ref, gd_s.at[q], gd_r.at[q], partner, t)

    def pair_send(q):
        for zz in range(nz):
            psend[q][zz] = part[q][(1 - c) * nz + zz].astype(BF16)
        pairs[q].start()

    def line_send(q):
        pairs[q].wait_recv()
        if q in chained:
            line_step(q, 0)
            return
        for pz in peers_z:
            zsend[q][pz] = (part[q][c * nz + pz] + pbuf[q][pz].astype(F32)).astype(BF16)
            line(q, pz).start()

    def line_sum(q):
        acc = part[q][me] + pbuf[q][z].astype(F32)
        if q in chained:
            for at in range(nz):
                @pl.when(z == at)
                def _():
                    sums = acc
                    if at > 0:
                        if at == nz - 1:
                            took(zbuf[q].at[pl.ds(0, 1)], z_r.at[q, 0])
                        sums = sums + zbuf[q][at].astype(F32)
                    if at < nz - 1:
                        if at == 0:
                            took(zbuf[q].at[pl.ds(0, 1)], z_r.at[q, 1])
                        sums = sums + zbuf[q][nz].astype(F32)
                    tot[q][at + c * nz] = sums.astype(BF16)
        else:
            took(zbuf[q].at[pl.ds(0, nz - 1)], z_r.at[q, 0])
            for pz in peers_z:
                acc = acc + zbuf[q][pz].astype(F32)
            tot[q][me] = acc.astype(BF16)
        for pz in peers_z:
            share(q, pz, me).start()

    def line_take(q):
        took(tot[q].at[pl.ds(0, nz - 1)], g_r.at[q])
        share_core(q).start()

    def direct(q):
        i, r = streams[q]
        if r == 0:
            fetch[8 + i].wait()
            fetch[10 + i].wait()
        share_core(q).wait_recv()
        at = pl.ds(r * half, half)
        proj = tot[q][...].astype(F32).reshape(half, tot[q].shape[2])
        mean_out = MEAN_DECAY * mean[i][at, :] + (1.0 - MEAN_DECAY) * proj
        square_out = BETA_SQUARE * square[i][at, :] + (1.0 - BETA_SQUARE) * proj * proj
        mean_new[i][at, :] = mean_out
        square_new[i][at, :] = square_out
        dirs[i][at, :] = (mean_out / jnp.sqrt(square_out)).astype(BF16)

    def norm(i):
        height = bg[i].shape[1]
        group = max(1, 1024 // height)
        sums = jnp.zeros((1, dirs[i].shape[1]), F32)
        for g in range(0, nf, group):
            some = bg[i][g:g + group]
            u = jnp.dot(some.reshape(some.shape[0] * height, rank), dirs[i][...], preferred_element_type=F32)
            full[i][g * height:(g + some.shape[0]) * height, :] = u
            sums = sums + jnp.sum(u * u, axis=0, keepdims=True)
        tile = jnp.zeros((8, 128), F32) + jnp.sum(sums, axis=1, keepdims=True)
        tsend[i] = tile
        tbuf[t, i] = tile

    def rest_send(i):
        def parts():
            for b in peers_z:
                for pt in peers_t:
                    @pl.when(pt != b)
                    def _():
                        rest_plane(i, b, t, pt).start()
        when_part(i, t, parts)

        @pl.when(elsewhere)
        def _():
            rest_core(i, f).start()

    def rest_take(i):
        for b in peers_z:
            @pl.when(b != t)
            def _():
                senders(i, lambda n: took_slabs(i, e_r.at[i, b], n))
                rest_core(i, b * CORES + c).start()

    def rest_end(i):
        took(bg[i].at[pl.ds(0, nz - 1)], cd_r.at[i])

    def basis_gone():
        for k, (i, first, size) in enumerate(chunks):
            def line_out(k=k, i=i, size=size):
                took_slabs(i, b_s.at[k], nz - 1, size=size)
                pl.when(elsewhere)(lambda: took_slabs(i, c_s.at[k], nz - 2, size=size))
                pl.when(own_column)(lambda: took_slabs(i, c_s.at[k], nz - 1, size=size))
            when_part(i, t, line_out)
            basis_core(k, lane).wait_send()

    def rest_gone():
        for i in PAIR:
            def rest_out(i=i):
                for b in peers_z:
                    pl.when(b == t)(lambda: took_slabs(i, e_s.at[i, b], nt - 1))
                    pl.when(b != t)(lambda: took_slabs(i, e_s.at[i, b], nt - 2))
            when_part(i, t, rest_out)
            took(bg[i].at[pl.ds(0, nz - 1)], cd_s.at[i])

    def tokens_gone(q):
        sent = 2 * sum(sizes[1:])
        took(lifted[q].at[pl.ds(0, sent)], rs_s.at[q])
        took(lifted[q].at[pl.ds(0, sent)], ag_s.at[q])

    def line_gone(q):
        pairs[q].wait_send()
        took(zsend[q].at[pl.ds(0, nz - 1)], z_s.at[q])
        took(tot[q].at[pl.ds(0, nz - 1)], g_s.at[q])
        share_core(q).wait_send()

    def weights_gone():
        for i in PAIR:
            took(wg[i].at[pl.ds(0, nz)], wd_s.at[i])
            for at in range(nz):
                @pl.when(z == at)
                def _():
                    if at < nz - 1:
                        took(wg[i].at[pl.ds(0, at + 1)], w_u.at[i])
                    if at > 0:
                        took(wg[i].at[pl.ds(0, nz - at)], w_d.at[i])

    for k in range(len(chunks)):
        basis_in(k)
    for k in range(len(chunks)):
        basis_joined(k)
    fetch[0].wait()
    basis_core(0, other).wait_recv()
    lift(0)
    basis_core(1, other).wait_recv()
    lift(1)
    for u in range(len(units)):
        w_core(u, z, c).start()
    fetch[1].wait()
    basis_core(2, other).wait_recv()
    halve(0, 0)
    lift(2)
    weights_on(NEAR[0])
    halve(1, 0)
    for k in range(1, levels - 1):
        for q in PAIR:
            halve(q, k)
    halve(0, levels - 1)
    lift(3)
    weights_on(NEAR[1])
    halve(1, levels - 1)
    for k in range(levels - 1, 0, -1):
        for q in PAIR:
            double(q, k)
    weights_on(NEAR[2])
    halve(2, 0)
    double(0, 0)
    pair_send(0)
    halve(3, 0)
    double(1, 0)
    pair_send(1)
    for k in range(1, levels - 1):
        for q in (2, 3):
            halve(q, k)
    line_send(0)
    halve(2, levels - 1)
    line_send(1)
    halve(3, levels - 1)
    weights_on(NEAR[3])
    for k in range(levels - 1, 0, -1):
        for q in (2, 3):
            double(q, k)
    line_step(0, 1)
    line_step(1, 1)
    weights_on(NEAR[4])
    double(2, 0)
    pair_send(2)
    for k in range(2, nz - 1):
        line_step(0, k)
        line_step(1, k)
    double(3, 0)
    pair_send(3)
    line_send(2)
    line_send(3)
    line_sum(0)
    line_sum(1)
    for i in PAIR:
        rest_send(i)
    weights_on(NEAR[5])
    basis_gone()
    tokens_gone(0)
    tokens_gone(1)
    line_sum(2)
    line_sum(3)
    weights_on(NEAR[6])
    line_take(0)
    line_take(1)
    for i in PAIR:
        rest_take(i)
    direct(0)
    direct(1)
    line_take(2)
    line_take(3)
    for i in PAIR:
        rest_end(i)
    norm(0)
    direct(2)
    direct(3)
    norm(1)
    for pt in peers_t:
        rcopy(tsend, tbuf.at[t], t_s.at[0], t_r.at[0], f, pt).start()
    rest_gone()
    tokens_gone(2)
    tokens_gone(3)
    for q in range(4):
        line_gone(q)
    weights_on([(s, u) for s in range(3, nz) for u in range(len(units))])
    took(tbuf.at[pl.ds(0, nt - 1)], t_r.at[0])
    summed = tbuf[0]
    for k in range(1, nt):
        summed = summed + tbuf[k]
    totals[...] = summed
    for i in PAIR:
        took(wg[i].at[pl.ds(0, nz)], wd_r.at[i])
    weights_gone()
    took(tbuf.at[pl.ds(0, nt - 1)], t_s.at[0])


def gather_and_reduce(nf, nt, lefts, rights, weights, bases, means, squares):
    rank, nz, tokens = bases[0].shape[1], nf // CORES, rights[0].shape[0]
    half, levels = rank // 2, nt.bit_length() - 1
    seg = half // nf
    heights, widths = [b.shape[0] for b in bases], [r.shape[1] for r in rights]
    units = sum(h // u for h, u in zip(heights, unit_heights(heights, widths)))
    vmem, dma = pl.BlockSpec(memory_space=pltpu.VMEM), pltpu.SemaphoreType.DMA
    hbm = pl.BlockSpec(memory_space=pltpu.HBM)

    def two(shape_of, kind=BF16, make=pltpu.VMEM):
        return [make(shape_of(h, w), kind) for h, w in zip(heights, widths)]

    def four(shape_of, kind=BF16):
        return [pltpu.VMEM(shape_of(w), kind) for w in widths for _ in PAIR]

    def outs(shape_of, kind=BF16):
        return two(shape_of, kind, jax.ShapeDtypeStruct)

    halves = lambda w: (2, tokens // 2, half)
    pieces = lambda w: (nz, seg, w)
    ranked = lambda h, w: (rank, w)
    fetched = (*lefts, *rights, *means, *squares)
    return pl.pallas_call(
        functools.partial(exchange, nf, nt),
        out_shape=(
            *outs(lambda h, w: (nf, h, w)), *outs(lambda h, w: (nf * h, w), F32),
            *outs(ranked, F32), *outs(ranked, F32), *outs(lambda h, w: (h, w), F32),
            jax.ShapeDtypeStruct((2, 8, 128), F32),
        ),
        in_specs=[hbm] * 12,
        out_specs=(vmem,) * 11,
        scratch_shapes=[
            *[pltpu.VMEM(x.shape, x.dtype) for x in fetched], *two(lambda h, w: (nf, h, rank)), *two(ranked),
            *four(halves), *four(halves), *four(halves, F32), *four(lambda w: (tokens, half)),
            *four(lambda w: (nf, seg, w), F32), *four(pieces), *four(pieces), *four(pieces),
            *four(lambda w: (nz + 1, seg, w)),
            *four(lambda w: (nf, seg, w)),
            pltpu.VMEM((2, 8, 128), F32),
            pltpu.VMEM((nt, 2, 8, 128), F32),
            dma((12,)), *[dma((3,))] * 6, *[dma((2, nz))] * 2, *[dma((2,))] * 2, dma((2,)), dma((2,)), dma((units, nz)), dma((2,)), dma((2,)),
            dma((4,)), dma((4, levels)), dma((4,)), dma((4, levels)), dma((4,)), dma((4,)), dma((4,)), dma((4, 2)),
            *[dma((4,))] * 4, dma((1,)), dma((1,)),
        ],
        compiler_params=pltpu.CompilerParams(
            collective_id=0, has_side_effects=True, vmem_limit_bytes=34 * 1024 * 1024
        ),
        name="exchange",
    )(*[pltpu.with_memory_space_constraint(x, pltpu.HBM)
        for x in (*lefts, *rights, *weights, *bases, *means, *squares)])


def apply(nf, nt, *refs):
    wg, full, mean_new, square_new, w32 = (refs[2 * k:2 * k + 2] for k in range(5))
    totals = refs[10]
    outs = [refs[11 + 5 * i:16 + 5 * i] for i in PAIR]
    step, new, copy = (refs[21 + 2 * k:23 + 2 * k] for k in range(3))
    sem, csem = refs[27:]
    f = lax.axis_index("fs")

    def to(k, i):
        src = (step, new, None, mean_new, square_new)[k]
        return pltpu.make_async_copy(src[i], outs[i][k], sem.at[i, k])

    def block(i, g):
        height = w32[i].shape[0]
        return pltpu.make_async_copy(copy[i].at[pl.ds(g * height, height)],
                                     outs[i][2].at[pl.ds(g * height, height)], csem.at[i, g])

    for i in PAIR:
        to(3, i).start()
        to(4, i).start()
    scales = []
    for i in PAIR:
        count = w32[i].shape[0] * nf * w32[i].shape[1] * nt
        scale = LEARN_RATE * lax.rsqrt(totals[i, 0:1, 0:1] / lax.convert_element_type(count, F32) + EPS_RMS)
        scales.append(scale)
        height = w32[i].shape[0]
        own = scale * full[i][pl.ds(pl.multiple_of(f * height, height), height), :]
        step[i][...] = own
        new[i][...] = w32[i][...] - own
        to(0, i).start()
        to(1, i).start()
    for i in PAIR:
        height = w32[i].shape[0]
        for g in range(nf):
            at = pl.ds(g * height, height)
            copy[i][at, :] = (wg[i][g].astype(F32) - scales[i] * full[i][at, :]).astype(BF16)
            block(i, g).start()
    for i in PAIR:
        for k in (0, 1, 3, 4):
            to(k, i).wait()
        for g in range(nf):
            block(i, g).wait()


def finish(nf, nt, gathered):
    w32 = gathered[8:10]
    vmem, hbm = pl.BlockSpec(memory_space=pltpu.VMEM), pl.BlockSpec(memory_space=pltpu.HBM)
    out_shape = []
    for i in PAIR:
        copy = jax.ShapeDtypeStruct((nf * w32[i].shape[0], w32[i].shape[1]), BF16)
        like = lambda x: jax.ShapeDtypeStruct(x.shape, F32)
        out_shape += [like(w32[i]), like(w32[i]), copy, like(gathered[4 + i]), like(gathered[6 + i])]
    return pl.pallas_call(
        functools.partial(apply, nf, nt),
        in_specs=[vmem] * 11,
        out_specs=[hbm] * 10,
        out_shape=out_shape,
        scratch_shapes=[
            *[pltpu.VMEM(w.shape, F32) for w in w32], *[pltpu.VMEM(w.shape, F32) for w in w32],
            *[pltpu.VMEM(out_shape[2 + 5 * i].shape, BF16) for i in PAIR],
            pltpu.SemaphoreType.DMA((2, 5)), pltpu.SemaphoreType.DMA((2, nf)),
        ],
        compiler_params=pltpu.CompilerParams(vmem_limit_bytes=12 * 1024 * 1024),
        name="apply",
    )(*gathered)


def per_device(nf, nt, attn_out, out_cot, latent, value_cot, out_weight, value_up_matrix,
               out_basis, value_basis, out_mean, out_square, value_mean, value_square):
    gathered = gather_and_reduce(
        nf, nt, (attn_out, latent), (out_cot, value_cot), (out_weight, value_up_matrix),
        (out_basis, value_basis), (out_mean, value_mean), (out_square, value_square))
    return tuple(finish(nf, nt, gathered))


def solution(mesh):
    both, rows, cols = P("fs", "tp"), P("fs", None), P(None, "tp")
    return jax.shard_map(
        functools.partial(per_device, mesh.shape["fs"], mesh.shape["tp"]),
        mesh=mesh,
        in_specs=(both,) * 6 + (rows,) * 2 + (cols,) * 4,
        out_specs=(both, both, cols, cols, cols) * 2,
        check_vma=False,
    )
```

```python
import functools

import jax
import jax.numpy as jnp
from jax import lax
from jax.experimental import pallas as pl
from jax.experimental.pallas import tpu as pltpu
from jax.sharding import PartitionSpec as P

LEARN_RATE = 0.01
MEAN_DECAY = 0.8
BETA_SQUARE = 0.9
EPS_RMS = 1e-06
MESH = pl.DeviceIdType.MESH
F32, BF16 = jnp.float32, jnp.bfloat16
PAIR = (0, 1)
CORES = 2
NEAR = (((1, 0), (1, 1)), ((1, 2), (1, 3)), ((1, 4), (2, 0)), ((2, 1),), ((2, 2),), (), ((2, 3), (2, 4)))


def rcopy(src, dst, send, recv, fs, tp):
    return pltpu.make_async_remote_copy(
        src_ref=src, dst_ref=dst, send_sem=send, recv_sem=recv,
        device_id=(fs, tp), device_id_type=MESH,
    )


def over_rows(left, right):
    return lax.dot_general(left, right, (((0,), (0,)), ((), ())), preferred_element_type=F32)


def unit_heights(heights, widths):
    least = min(h * w for h, w in zip(heights, widths))
    return [least // w for w in widths]


def parts_of(height, nt):
    return min(nt, height // 16)


def exchange(nf, nt, *refs):
    hbm, rest = refs[:12], refs[12:]
    wg, full, mean_new, square_new, w32 = (rest[2 * k:2 * k + 2] for k in range(5))
    totals, rest = rest[10], rest[11:]
    left, right, mean, square, bg, dirs = (rest[2 * k:2 * k + 2] for k in range(6))
    sbuf, rbuf, kept, lifted, part, psend, pbuf, zsend, zbuf, tot = (rest[12 + 4 * k:16 + 4 * k] for k in range(10))
    (tsend, tbuf, isem, b_s, b_r, bd_s, bd_r, c_s, c_r, e_s, e_r, cd_s, cd_r, w_u, w_d, w_r, wd_s, wd_r,
     rs_s, rs_r, ag_r, p_r, z_s, z_r, g_r, gd_r, t_s, t_r) = rest[52:]

    nz = nf // CORES
    f, t = lax.axis_index("fs"), lax.axis_index("tp")
    z, c = lax.div(f, CORES), lax.rem(f, CORES)
    partner = f + 1 - 2 * c
    rank = bg[0].shape[2]
    half = rank // 2
    tokens = left[0].shape[0]
    peers_t = [lax.rem(t + s, nt) for s in range(1, nt)]
    peers_z = [lax.rem(z + s, nz) for s in range(1, nz)]
    own_column = z == t
    elsewhere = jnp.logical_not(own_column)

    held = (*left, *right, *w32, *[b.at[f] for b in bg], *mean, *square)
    order = (6, 7, 4, 5, 0, 1, 2, 3, 8, 9, 10, 11)
    fetch = [pltpu.make_async_copy(hbm[k], held[k], isem.at[k]) for k in range(12)]
    for k in order:
        fetch[k].start()

    barrier = pltpu.get_barrier_semaphore()
    pl.semaphore_signal(barrier, inc=1, device_id=(partner, t), device_id_type=MESH)
    for pz in peers_z:
        pl.semaphore_signal(barrier, inc=1, device_id=(pz * CORES + c, t), device_id_type=MESH)
    for pt in peers_t:
        pl.semaphore_signal(barrier, inc=1, device_id=(f, pt), device_id_type=MESH)
    pl.semaphore_wait(barrier, 1 + len(peers_z) + len(peers_t))

    def took(ref, sem):
        pltpu.make_async_copy(ref, ref, sem).wait()

    def took_slabs(k_or_i, sem, count, first=0, size=None):
        size = rank if size is None else size
        i = k_or_i
        tall = bg[i].shape[1] // parts_of(bg[i].shape[1], nt)
        took(lifted[0].at[pl.ds(0, count * tall * size // half)], sem)

    lane = t * CORES + c
    other = t * CORES + 1 - c
    chunks = ((0, 0, half), (0, half, half), (1, 0, rank))

    def slab(i, block, column, first=0, size=rank):
        tall = bg[i].shape[1] // parts_of(bg[i].shape[1], nt)
        return bg[i].at[block, pl.ds(pl.multiple_of(column * tall, tall), tall), pl.ds(first, size)]

    def when_part(i, column, then):
        parts = parts_of(bg[i].shape[1], nt)
        if parts == nt:
            then()
        else:
            pl.when(column < parts)(then)

    def basis_line(k, pz, block):
        i, first, size = chunks[k]
        ref = slab(i, block, t, first, size)
        return rcopy(ref, ref, b_s.at[k], b_r.at[k], pz * CORES + c, t)

    def basis_plane(k, b, column):
        i, first, size = chunks[k]
        ref = slab(i, b * CORES + c, column, first, size)
        return rcopy(ref, ref, c_s.at[k], c_r.at[k], f, b)

    def basis_core(k, block):
        i, first, size = chunks[k]
        ref = bg[i].at[block, :, pl.ds(first, size)]
        return rcopy(ref, ref, bd_s.at[k], bd_r.at[k], partner, t)

    def rest_plane(i, b, column, pt):
        ref = slab(i, b * CORES + c, column)
        return rcopy(ref, ref, e_s.at[i, b], e_r.at[i, b], f, pt)

    def rest_core(i, block):
        ref = bg[i].at[block]
        return rcopy(ref, ref, cd_s.at[i], cd_r.at[i], partner, t)

    heights = [w.shape[1] for w in wg]
    tall = unit_heights(heights, [w.shape[2] for w in wg])
    units = [(i, r) for i in PAIR for r in range(0, heights[i], tall[i])]

    def unit(u, zb, core):
        i, r = units[u]
        return wg[i].at[zb * CORES + core, pl.ds(r, tall[i])]

    def w_up(u, zb):
        ref = unit(u, zb, c)
        return rcopy(ref, ref, w_u.at[units[u][0]], w_r.at[u, zb], f + CORES, t)

    def w_dn(u, zb):
        ref = unit(u, zb, c)
        return rcopy(ref, ref, w_d.at[units[u][0]], w_r.at[u, zb], f - CORES, t)

    def w_core(u, zb, core):
        ref = unit(u, zb, core)
        return rcopy(ref, ref, wd_s.at[units[u][0]], wd_r.at[units[u][0]], partner, t)

    def weights_on(events):
        for s, u in events:
            if s > nz - 1:
                continue

            @pl.when(z >= s)
            def _():
                w_up(u, z - s).wait_recv()

                @pl.when(z < nz - 1)
                def _():
                    w_up(u, z - s).start()
                w_core(u, z - s, c).start()

            @pl.when(z + s <= nz - 1)
            def _():
                w_dn(u, z + s).wait_recv()

                @pl.when(z > 0)
                def _():
                    w_dn(u, z + s).start()
                w_core(u, z + s, c).start()

    fetch[6].wait()
    fetch[7].wait()
    for k in range(len(chunks)):
        def to_line(k=k):
            for pz in [lax.rem(z + s, nz) for s in range(nz // 2, nz)] + [lax.rem(z + s, nz) for s in range(1, nz // 2)]:
                basis_line(k, pz, f).start()
        when_part(chunks[k][0], t, to_line)

    @pl.when(own_column)
    def _():
        for k in range(len(chunks)):
            basis_core(k, lane).start()
    for i in PAIR:
        fetch[4 + i].wait()
        wg[i][f] = w32[i][...].astype(BF16)
    for u in range(len(units)):
        @pl.when(z < nz - 1)
        def _():
            w_up(u, z).start()

        @pl.when(z > 0)
        def _():
            w_dn(u, z).start()

    levels = nt.bit_length() - 1
    sizes = [tokens // 2 >> k for k in range(levels + 1)]
    offs = [sizes[0] - s for s in sizes]
    masks = [[1 << k for k in range(levels)], [1 << k for k in reversed(range(levels))]]
    bits = [[lax.rem(lax.div(t, m), 2) for m in masks[h]] for h in PAIR]
    mates = [[t + m * (1 - 2 * b) for m, b in zip(masks[h], bits[h])] for h in PAIR]
    bases = []
    for h in PAIR:
        at = [h * sizes[0]]
        for k in range(levels):
            at.append(at[-1] + bits[h][k] * sizes[k + 1])
        bases.append(at)
    streams = tuple((i, r) for i in PAIR for r in PAIR)

    def rows(start, size):
        return pl.ds(pl.multiple_of(start, 16), size)

    def away(h, k):
        return rows(bases[h][k] + (1 - bits[h][k]) * sizes[k + 1], sizes[k + 1])

    def rs(q, h, k):
        at = pl.ds(offs[k], sizes[k + 1])
        return rcopy(sbuf[q].at[h, at], rbuf[q].at[h, at], rs_s.at[q], rs_r.at[q, k], f, mates[h][k])

    def ag(q, h, k):
        ref = lifted[q].at[rows(bases[h][k + 1], sizes[k + 1])]
        return rcopy(ref, ref, rs_s.at[q], ag_r.at[q, k], f, mates[h][k])

    def senders(i, then):
        parts = parts_of(bg[i].shape[1], nt)
        if parts == nt:
            then(nt - 1)
        else:
            pl.when(t < parts)(lambda: then(parts - 1))
            pl.when(t >= parts)(lambda: then(parts))

    def basis_in(k):
        i, first, size = chunks[k]

        def from_line():
            took_slabs(i, b_r.at[k], nz - 1, size=size)
            for b in peers_z:
                @pl.when(b != t)
                def _():
                    basis_plane(k, b, t).start()

        when_part(i, t, from_line)

    def basis_joined(k):
        i, first, size = chunks[k]

        @pl.when(elsewhere)
        def _():
            senders(i, lambda n: took_slabs(i, c_r.at[k], n, size=size))
            basis_core(k, lane).start()

    def lift(q):
        i, r = streams[q]
        two = bg[i][pl.ds(t * CORES, CORES), :, r * half:(r + 1) * half]
        factor = two.reshape(two.shape[0] * two.shape[1], half)
        for h in PAIR:
            sbuf[q][h, pl.ds(0, sizes[1])] = jnp.dot(
                left[i][away(h, 0), :], factor, preferred_element_type=F32).astype(BF16)
            rs(q, h, 0).start()
        for h in PAIR:
            kept[q][h, pl.ds(0, sizes[1])] = jnp.dot(
                left[i][rows(bases[h][1], sizes[1]), :], factor, preferred_element_type=F32)

    def contract(q, at, first=False):
        i = streams[q][0]
        got = over_rows(lifted[q][at, :], right[i][at, :]).reshape(part[q].shape)
        if first:
            part[q][...] = got
        else:
            part[q][...] += got

    def halve(q, k):
        took(rbuf[q].at[:, pl.ds(offs[k], sizes[k + 1])], rs_r.at[q, k])
        for h in PAIR:
            if k + 1 < levels:
                small = sizes[k + 2]
                for b, mine in ((1 - bits[h][k + 1], False), (bits[h][k + 1], True)):
                    at = rows(offs[k] + b * small, small)
                    both = kept[q][h, at] + rbuf[q][h, at].astype(F32)
                    to = pl.ds(offs[k + 1], small)
                    if mine:
                        kept[q][h, to] = both
                    else:
                        sbuf[q][h, to] = both.astype(BF16)
                        rs(q, h, k + 1).start()
            else:
                at = pl.ds(offs[k], sizes[k + 1])
                lifted[q][rows(bases[h][k + 1], sizes[k + 1]), :] = (
                    kept[q][h, at] + rbuf[q][h, at].astype(F32)).astype(BF16)
                ag(q, h, k).start()
        if k + 1 == levels:
            i, r = streams[q]
            if r == 0:
                fetch[2 + i].wait()
            for h in PAIR:
                contract(q, rows(bases[h][levels], sizes[levels]), h == 0)

    def double(q, k):
        took(lifted[q].at[pl.ds(0, 2 * sizes[k + 1])], ag_r.at[q, k])
        if k > 0:
            for h in PAIR:
                ag(q, h, k - 1).start()
        for h in PAIR:
            contract(q, away(h, k))

    pairs = [rcopy(psend[q], pbuf[q], z_s.at[q], p_r.at[q], partner, t) for q in range(4)]
    me = c * nz + z

    chained = (0, 1)

    def line(q, pz):
        return rcopy(zsend[q].at[pz], zbuf[q].at[z], z_s.at[q], z_r.at[q, 0], pz * CORES + c, t)

    def hop(q, zz, up, slot):
        return rcopy(zsend[q].at[zz], zbuf[q].at[slot], z_s.at[q], z_r.at[q, 0 if up else 1],
                     f + (CORES if up else -CORES), t)

    def line_step(q, k):
        for at, up in ((k, True), (nz - 1 - k, False)):
            @pl.when(z == at)
            def _():
                if k > 0:
                    took(zbuf[q].at[pl.ds(0, nz - k)], z_r.at[q, 0 if up else 1])
                for zz in (range(at + 1, nz) if up else range(at)):
                    sums = part[q][c * nz + zz] + pbuf[q][zz].astype(F32)
                    if k > 0:
                        sums = sums + zbuf[q][zz].astype(F32)
                    zsend[q][zz] = sums.astype(BF16)
                    beside = at + 1 if up else at - 1
                    hop(q, zz, up, nz if zz == beside and not up else zz).start()

    def share(q, pz, at):
        ref = tot[q].at[at]
        return rcopy(ref, ref, z_s.at[q], g_r.at[q], pz * CORES + c, t)

    def share_core(q):
        ref = tot[q].at[pl.ds(c * nz, nz)]
        return rcopy(ref, ref, z_s.at[q], gd_r.at[q], partner, t)

    def pair_send(q):
        for zz in range(nz):
            psend[q][zz] = part[q][(1 - c) * nz + zz].astype(BF16)
        pairs[q].start()

    def line_send(q):
        pairs[q].wait_recv()
        if q in chained:
            line_step(q, 0)
            return
        for pz in peers_z:
            zsend[q][pz] = (part[q][c * nz + pz] + pbuf[q][pz].astype(F32)).astype(BF16)
            line(q, pz).start()

    def line_sum(q):
        acc = part[q][me] + pbuf[q][z].astype(F32)
        if q in chained:
            for at in range(nz):
                @pl.when(z == at)
                def _():
                    sums = acc
                    if at > 0:
                        if at == nz - 1:
                            took(zbuf[q].at[pl.ds(0, 1)], z_r.at[q, 0])
                        sums = sums + zbuf[q][at].astype(F32)
                    if at < nz - 1:
                        if at == 0:
                            took(zbuf[q].at[pl.ds(0, 1)], z_r.at[q, 1])
                        sums = sums + zbuf[q][nz].astype(F32)
                    tot[q][at + c * nz] = sums.astype(BF16)
        else:
            took(zbuf[q].at[pl.ds(0, nz - 1)], z_r.at[q, 0])
            for pz in peers_z:
                acc = acc + zbuf[q][pz].astype(F32)
            tot[q][me] = acc.astype(BF16)
        for pz in peers_z:
            share(q, pz, me).start()

    def line_take(q):
        took(tot[q].at[pl.ds(0, nz - 1)], g_r.at[q])
        share_core(q).start()

    def direct(q):
        i, r = streams[q]
        if r == 0:
            fetch[8 + i].wait()
            fetch[10 + i].wait()
        share_core(q).wait_recv()
        at = pl.ds(r * half, half)
        proj = tot[q][...].astype(F32).reshape(half, tot[q].shape[2])
        mean_out = MEAN_DECAY * mean[i][at, :] + (1.0 - MEAN_DECAY) * proj
        square_out = BETA_SQUARE * square[i][at, :] + (1.0 - BETA_SQUARE) * proj * proj
        mean_new[i][at, :] = mean_out
        square_new[i][at, :] = square_out
        dirs[i][at, :] = (mean_out / jnp.sqrt(square_out)).astype(BF16)

    def norm(i):
        height = bg[i].shape[1]
        group = max(1, 1024 // height)
        sums = jnp.zeros((1, dirs[i].shape[1]), F32)
        for g in range(0, nf, group):
            some = bg[i][g:g + group]
            u = jnp.dot(some.reshape(some.shape[0] * height, rank), dirs[i][...], preferred_element_type=F32)
            full[i][g * height:(g + some.shape[0]) * height, :] = u
            sums = sums + jnp.sum(u * u, axis=0, keepdims=True)
        tile = jnp.zeros((8, 128), F32) + jnp.sum(sums, axis=1, keepdims=True)
        tsend[i] = tile
        tbuf[t, i] = tile

    def rest_send(i):
        def parts():
            for b in peers_z:
                for pt in peers_t:
                    @pl.when(pt != b)
                    def _():
                        rest_plane(i, b, t, pt).start()
        when_part(i, t, parts)

        @pl.when(elsewhere)
        def _():
            rest_core(i, f).start()

    def rest_take(i):
        for b in peers_z:
            @pl.when(b != t)
            def _():
                senders(i, lambda n: took_slabs(i, e_r.at[i, b], n))
                rest_core(i, b * CORES + c).start()

    def rest_end(i):
        took(bg[i].at[pl.ds(0, nz - 1)], cd_r.at[i])

    def basis_gone():
        for k, (i, first, size) in enumerate(chunks):
            def line_out(k=k, i=i, size=size):
                took_slabs(i, b_s.at[k], nz - 1, size=size)
                pl.when(elsewhere)(lambda: took_slabs(i, c_s.at[k], nz - 2, size=size))
                pl.when(own_column)(lambda: took_slabs(i, c_s.at[k], nz - 1, size=size))
            when_part(i, t, line_out)
            basis_core(k, lane).wait_send()

    def rest_gone():
        for i in PAIR:
            def rest_out(i=i):
                for b in peers_z:
                    pl.when(b == t)(lambda: took_slabs(i, e_s.at[i, b], nt - 1))
                    pl.when(b != t)(lambda: took_slabs(i, e_s.at[i, b], nt - 2))
            when_part(i, t, rest_out)
            took(bg[i].at[pl.ds(0, nz - 1)], cd_s.at[i])

    def tokens_gone(q):
        sent = 2 * sum(sizes[1:])
        took(kept[q].at[:, pl.ds(0, sent // 2)], rs_s.at[q])

    def line_gone(q):
        took(part[q].at[pl.ds(0, 2 * nz - 1)], z_s.at[q])

    def weights_gone():
        for i in PAIR:
            took(wg[i].at[pl.ds(0, nz)], wd_s.at[i])
            for at in range(nz):
                @pl.when(z == at)
                def _():
                    if at < nz - 1:
                        took(wg[i].at[pl.ds(0, at + 1)], w_u.at[i])
                    if at > 0:
                        took(wg[i].at[pl.ds(0, nz - at)], w_d.at[i])

    for k in range(len(chunks)):
        basis_in(k)
    for k in range(len(chunks)):
        basis_joined(k)
    fetch[0].wait()
    basis_core(0, other).wait_recv()
    lift(0)
    basis_core(1, other).wait_recv()
    lift(1)
    for u in range(len(units)):
        w_core(u, z, c).start()
    fetch[1].wait()
    basis_core(2, other).wait_recv()
    halve(0, 0)
    lift(2)
    weights_on(NEAR[0])
    halve(1, 0)
    for k in range(1, levels - 1):
        for q in PAIR:
            halve(q, k)
    halve(0, levels - 1)
    lift(3)
    weights_on(NEAR[1])
    halve(1, levels - 1)
    for k in range(levels - 1, 0, -1):
        for q in PAIR:
            double(q, k)
    weights_on(NEAR[2])
    halve(2, 0)
    double(0, 0)
    pair_send(0)
    halve(3, 0)
    double(1, 0)
    pair_send(1)
    for k in range(1, levels - 1):
        for q in (2, 3):
            halve(q, k)
    line_send(0)
    halve(2, levels - 1)
    line_send(1)
    halve(3, levels - 1)
    weights_on(NEAR[3])
    for k in range(levels - 1, 0, -1):
        for q in (2, 3):
            double(q, k)
    line_step(0, 1)
    line_step(1, 1)
    weights_on(NEAR[4])
    double(2, 0)
    pair_send(2)
    for k in range(2, nz - 1):
        line_step(0, k)
        line_step(1, k)
    double(3, 0)
    pair_send(3)
    line_send(2)
    line_send(3)
    line_sum(0)
    line_sum(1)
    for i in PAIR:
        rest_send(i)
    weights_on(NEAR[5])
    basis_gone()
    tokens_gone(0)
    tokens_gone(1)
    line_sum(2)
    line_sum(3)
    weights_on(NEAR[6])
    line_take(0)
    line_take(1)
    for i in PAIR:
        rest_take(i)
    direct(0)
    direct(1)
    line_take(2)
    line_take(3)
    for i in PAIR:
        rest_end(i)
    norm(0)
    direct(2)
    direct(3)
    norm(1)
    for pt in peers_t:
        rcopy(tsend, tbuf.at[t], t_s.at[0], t_r.at[0], f, pt).start()
    rest_gone()
    tokens_gone(2)
    tokens_gone(3)
    for q in range(4):
        line_gone(q)
    weights_on([(s, u) for s in range(3, nz) for u in range(len(units))])
    took(tbuf.at[pl.ds(0, nt - 1)], t_r.at[0])
    summed = tbuf[0]
    for k in range(1, nt):
        summed = summed + tbuf[k]
    totals[...] = summed
    for i in PAIR:
        took(wg[i].at[pl.ds(0, nz)], wd_r.at[i])
    weights_gone()
    took(tbuf.at[pl.ds(0, nt - 1)], t_s.at[0])


def gather_and_reduce(nf, nt, lefts, rights, weights, bases, means, squares):
    rank, nz, tokens = bases[0].shape[1], nf // CORES, rights[0].shape[0]
    half, levels = rank // 2, nt.bit_length() - 1
    seg = half // nf
    heights, widths = [b.shape[0] for b in bases], [r.shape[1] for r in rights]
    units = sum(h // u for h, u in zip(heights, unit_heights(heights, widths)))
    vmem, dma = pl.BlockSpec(memory_space=pltpu.VMEM), pltpu.SemaphoreType.DMA
    hbm = pl.BlockSpec(memory_space=pltpu.HBM)

    def two(shape_of, kind=BF16, make=pltpu.VMEM):
        return [make(shape_of(h, w), kind) for h, w in zip(heights, widths)]

    def four(shape_of, kind=BF16):
        return [pltpu.VMEM(shape_of(w), kind) for w in widths for _ in PAIR]

    def outs(shape_of, kind=BF16):
        return two(shape_of, kind, jax.ShapeDtypeStruct)

    halves = lambda w: (2, tokens // 2, half)
    pieces = lambda w: (nz, seg, w)
    ranked = lambda h, w: (rank, w)
    fetched = (*lefts, *rights, *means, *squares)
    return pl.pallas_call(
        functools.partial(exchange, nf, nt),
        out_shape=(
            *outs(lambda h, w: (nf, h, w)), *outs(lambda h, w: (nf * h, w), F32),
            *outs(ranked, F32), *outs(ranked, F32), *outs(lambda h, w: (h, w), F32),
            jax.ShapeDtypeStruct((2, 8, 128), F32),
        ),
        in_specs=[hbm] * 12,
        out_specs=(vmem,) * 11,
        scratch_shapes=[
            *[pltpu.VMEM(x.shape, x.dtype) for x in fetched], *two(lambda h, w: (nf, h, rank)), *two(ranked),
            *four(halves), *four(halves), *four(halves, F32), *four(lambda w: (tokens, half)),
            *four(lambda w: (nf, seg, w), F32), *four(pieces), *four(pieces), *four(pieces),
            *four(lambda w: (nz + 1, seg, w)),
            *four(lambda w: (nf, seg, w)),
            pltpu.VMEM((2, 8, 128), F32),
            pltpu.VMEM((nt, 2, 8, 128), F32),
            dma((12,)), *[dma((3,))] * 6, *[dma((2, nz))] * 2, *[dma((2,))] * 2, dma((2,)), dma((2,)), dma((units, nz)), dma((2,)), dma((2,)),
            dma((4,)), dma((4, levels)), dma((4, levels)), dma((4,)), dma((4,)), dma((4, 2)),
            *[dma((4,))] * 2, dma((1,)), dma((1,)),
        ],
        compiler_params=pltpu.CompilerParams(
            collective_id=0, has_side_effects=True, vmem_limit_bytes=34 * 1024 * 1024
        ),
        name="exchange",
    )(*[pltpu.with_memory_space_constraint(x, pltpu.HBM)
        for x in (*lefts, *rights, *weights, *bases, *means, *squares)])


def apply(nf, nt, *refs):
    wg, full, mean_new, square_new, w32 = (refs[2 * k:2 * k + 2] for k in range(5))
    totals = refs[10]
    outs = [refs[11 + 5 * i:16 + 5 * i] for i in PAIR]
    step, new, copy = (refs[21 + 2 * k:23 + 2 * k] for k in range(3))
    sem, csem = refs[27:]
    f = lax.axis_index("fs")

    def to(k, i):
        src = (step, new, None, mean_new, square_new)[k]
        return pltpu.make_async_copy(src[i], outs[i][k], sem.at[i, k])

    def block(i, g):
        height = w32[i].shape[0]
        return pltpu.make_async_copy(copy[i].at[pl.ds(g * height, height)],
                                     outs[i][2].at[pl.ds(g * height, height)], csem.at[i, g])

    for i in PAIR:
        to(3, i).start()
        to(4, i).start()
    scales = []
    for i in PAIR:
        count = w32[i].shape[0] * nf * w32[i].shape[1] * nt
        scale = LEARN_RATE * lax.rsqrt(totals[i, 0:1, 0:1] / lax.convert_element_type(count, F32) + EPS_RMS)
        scales.append(scale)
        height = w32[i].shape[0]
        own = scale * full[i][pl.ds(pl.multiple_of(f * height, height), height), :]
        step[i][...] = own
        new[i][...] = w32[i][...] - own
        to(0, i).start()
        to(1, i).start()
    for i in PAIR:
        height = w32[i].shape[0]
        for g in range(nf):
            at = pl.ds(g * height, height)
            copy[i][at, :] = (wg[i][g].astype(F32) - scales[i] * full[i][at, :]).astype(BF16)
            block(i, g).start()
    for i in PAIR:
        for k in (0, 1, 3, 4):
            to(k, i).wait()
        for g in range(nf):
            block(i, g).wait()


def finish(nf, nt, gathered):
    w32 = gathered[8:10]
    vmem, hbm = pl.BlockSpec(memory_space=pltpu.VMEM), pl.BlockSpec(memory_space=pltpu.HBM)
    out_shape = []
    for i in PAIR:
        copy = jax.ShapeDtypeStruct((nf * w32[i].shape[0], w32[i].shape[1]), BF16)
        like = lambda x: jax.ShapeDtypeStruct(x.shape, F32)
        out_shape += [like(w32[i]), like(w32[i]), copy, like(gathered[4 + i]), like(gathered[6 + i])]
    return pl.pallas_call(
        functools.partial(apply, nf, nt),
        in_specs=[vmem] * 11,
        out_specs=[hbm] * 10,
        out_shape=out_shape,
        scratch_shapes=[
            *[pltpu.VMEM(w.shape, F32) for w in w32], *[pltpu.VMEM(w.shape, F32) for w in w32],
            *[pltpu.VMEM(out_shape[2 + 5 * i].shape, BF16) for i in PAIR],
            pltpu.SemaphoreType.DMA((2, 5)), pltpu.SemaphoreType.DMA((2, nf)),
        ],
        compiler_params=pltpu.CompilerParams(vmem_limit_bytes=12 * 1024 * 1024),
        name="apply",
    )(*gathered)


def per_device(nf, nt, attn_out, out_cot, latent, value_cot, out_weight, value_up_matrix,
               out_basis, value_basis, out_mean, out_square, value_mean, value_square):
    gathered = gather_and_reduce(
        nf, nt, (attn_out, latent), (out_cot, value_cot), (out_weight, value_up_matrix),
        (out_basis, value_basis), (out_mean, value_mean), (out_square, value_square))
    return tuple(finish(nf, nt, gathered))


def solution(mesh):
    both, rows, cols = P("fs", "tp"), P("fs", None), P(None, "tp")
    return jax.shard_map(
        functools.partial(per_device, mesh.shape["fs"], mesh.shape["tp"]),
        mesh=mesh,
        in_specs=(both,) * 6 + (rows,) * 2 + (cols,) * 4,
        out_specs=(both, both, cols, cols, cols) * 2,
        check_vma=False,
    )
```
